128 devices in a mesh: sp: 32 (over z, y, core), tp: 4 (over x).
Axes of the slice: x: 4, y: 4, z: 4, core: 2. Of those that a mesh axis runs over, the one named last changes fastest.
Arguments:
- stream: bfloat16 [8192, 2048], P(('sp', 'tp')), may hold values from -6 to 6
- queries: bfloat16 [8192, 2048], P('sp', 'tp'), may hold values from -147.07821 to 147.07821
- keys: bfloat16 [8192, 2048], P('sp', 'tp'), may hold values from -7 to 7
- values: bfloat16 [8192, 2048], P('sp', 'tp'), may hold values from -6 to 6
- head_lambda: float32 [8], P('tp'), may hold values from 0.3 to 0.8
- head_gain: float32 [256], replicated, may hold values from 0.1 to 1.9
- w_out: bfloat16 [2048, 2048], P('tp'), may hold values from -0.125 to 0.125
- norm_gain: float32 [2048], replicated, may hold values from 0.1 to 1.9
- w_gate: bfloat16 [2048, 5632], P('sp', 'tp'), may hold values from -0.125 to 0.125
- w_up: bfloat16 [2048, 5632], P('sp', 'tp'), may hold values from -0.125 to 0.125
- w_down: bfloat16 [5632, 2048], P('tp', 'sp'), may hold values from -0.078125 to 0.078125
Outputs:
- result: bfloat16 [8192, 2048], P(('sp', 'tp'))
The draws below stay inside these ranges and needn't reach their ends.
All inputs are finite; a program needn't handle non-finite values.
Results may differ from the reference program's by a relative error of at most 0.013.
Values may be sent and summed in bfloat16 or wider, within the bound.
No kernel may reach another device: no remote copies, remote signals or barrier semaphores. Data moves between devices by JAX's collectives and lax.ppermute only.
A program may use at most 192 MiB of HBM per device.

```python
import math
import jax
import jax.numpy as jnp
from jax import lax

D = 2048
H = 8
DH = 128
DV = 256
FF = 5632
TOKENS = 8192


def paired_draw(key):
    base_keys = jnp.clip(jax.random.normal(jax.random.fold_in(key, 11), (TOKENS, 2 * H * DH), jnp.float32), -6.0, 6.0)
    base_queries = 1.7 * jnp.clip(jax.random.normal(jax.random.fold_in(key, 12), (TOKENS, 2 * H * DH), jnp.float32), -6.0, 6.0)
    key_out = base_keys
    query_out = base_queries
    return (query_out, key_out)


def draw_queries(key, part):
    return paired_draw(key)[0].astype(jnp.bfloat16)


def draw_keys(key, part):
    return paired_draw(key)[1].astype(jnp.bfloat16)


def levels(own_key, extent, shards, smallest, largest):
    def one(dim, parts):
        draws = jax.random.uniform(jax.random.fold_in(jax.random.fold_in(own_key, 6), dim), (parts,), jnp.float32, smallest / len(shards), largest / len(shards))
        return jnp.repeat(jnp.exp(draws), extent[dim] // parts).reshape((-1,) + (1,) * (len(extent) - dim - 1))

    factor_of = one(*shards[0])
    for cut in shards[1:]:
        factor_of = factor_of * one(*cut)
    return factor_of


def scatter_about(key, shape, spread, limit, cuts=(), kind=jnp.bfloat16):
    entries = spread * jax.random.normal(key, shape, jnp.float32)
    if cuts:
        entries = entries * levels(key, shape, cuts, -0.22, 0.18)
    return jnp.clip(entries, -limit, limit).astype(kind)


def setup_inputs(seed: int = 0) -> dict:
    key_list = jax.random.split(jax.random.key(seed), 12)
    stream = scatter_about(key_list[0], (TOKENS, D), 1.0, 6.0, ((0, 128),))
    queries = draw_queries(jax.random.fold_in(key_list[11], 71), 0)
    keys = draw_keys(jax.random.fold_in(key_list[11], 71), 0)
    values = scatter_about(key_list[3], (TOKENS, H * DV), 1.0, 6.0, ((0, 32), (1, 4)))
    head_lambda = jnp.clip(0.3 + 0.5 * jax.random.uniform(key_list[4], (H,), jnp.float32) ** levels(key_list[4], (H,), ((0, 4),), -0.2, 0.2), 0.3, 0.8)
    head_gain = jnp.clip(1.0 + 0.18 * jax.random.normal(key_list[5], (DV,), jnp.float32), 0.1, 1.9)
    w_out = scatter_about(key_list[6], (H * DV, D), (H * DV) ** -0.5, 0.125, ((0, 4),))
    norm_gain = jnp.clip(1.0 + 0.18 * jax.random.normal(key_list[7], (D,), jnp.float32), 0.1, 1.9)
    w_gate = scatter_about(key_list[8], (D, FF), D ** -0.5, 0.125, ((0, 32), (1, 4)))
    w_up = scatter_about(key_list[9], (D, FF), D ** -0.5, 0.125, ((0, 32), (1, 4)))
    w_down = scatter_about(key_list[10], (FF, D), FF ** -0.5, 0.078125, ((0, 4), (1, 32)))
    return {"stream": stream, "queries": queries, "keys": keys, "values": values, "head_lambda": head_lambda, "head_gain": head_gain, "w_out": w_out, "norm_gain": norm_gain, "w_gate": w_gate, "w_up": w_up, "w_down": w_down}


epsilon = 1e-06

def normalize(values_in, gain):
    square_mean = lax.optimization_barrier(jnp.mean(values_in * values_in, axis=-1, keepdims=True))
    return values_in * lax.rsqrt(square_mean + epsilon) * gain

def reference(stream, queries, keys, values, head_lambda, head_gain, w_out, norm_gain, w_gate, w_up, w_down):
    token_count = queries.shape[0]
    query_heads = queries.reshape(token_count, H, 2, DH)
    key_heads = keys.reshape(token_count, H, 2, DH).astype(jnp.float32)
    value_heads = values.reshape(token_count, H, DV).astype(jnp.float32)
    block_rows = math.gcd(token_count, 256)
    key_pos = jnp.arange(token_count, dtype=jnp.int32)
    score_scale = DH ** (-0.5)

    def one_block(block_index):
        query_block = lax.dynamic_slice_in_dim(query_heads, (block_index * block_rows).astype(jnp.int32), block_rows, 0).astype(jnp.float32)
        scores = jnp.einsum('qhsd,khsd->hsqk', query_block, key_heads) * score_scale
        query_pos = block_index * block_rows + jnp.arange(block_rows, dtype=jnp.int32)
        visible = key_pos[None, :] <= query_pos[:, None]
        row_max = lax.optimization_barrier(jnp.max(jnp.where(visible, scores, -1e+30), axis=-1, keepdims=True))
        weights = jnp.where(visible, jnp.exp(scores - row_max), 0.0)
        weight_sum = lax.optimization_barrier(jnp.sum(weights, axis=-1))
        rounded = lax.optimization_barrier(weights.astype(jnp.bfloat16)).astype(jnp.float32)
        map_out = jnp.einsum('hsqk,khd->hsqd', rounded, value_heads) / weight_sum[..., None]
        contrast = map_out[:, 0] - head_lambda[:, None, None] * map_out[:, 1]
        normed_heads = normalize(contrast, head_gain)
        return normed_heads.transpose(1, 0, 2).reshape(block_rows, H * DV).astype(jnp.bfloat16)
    head_out = lax.map(one_block, jnp.arange(token_count // block_rows, dtype=jnp.int32)).reshape(token_count, H * DV)
    middle = stream.astype(jnp.float32) + jnp.dot(head_out, w_out, preferred_element_type=jnp.float32)
    normed = normalize(middle, norm_gain).astype(jnp.bfloat16)
    gate = jnp.dot(normed, w_gate, preferred_element_type=jnp.float32)
    up_part = jnp.dot(normed, w_up, preferred_element_type=jnp.float32)
    hidden = (jax.nn.silu(gate) * up_part).astype(jnp.bfloat16)
    mixed = jnp.dot(hidden, w_down, preferred_element_type=jnp.float32)
    return (middle + mixed).astype(jnp.bfloat16)
```

```python
import functools

import jax
import jax.numpy as jnp
import numpy as np
from jax import lax
from jax.experimental import pallas as pl
from jax.experimental.pallas import tpu as pltpu
from jax.sharding import PartitionSpec as P


EPS = 1e-6
NEG = -1e30
F32 = jnp.float32
BF16 = jnp.bfloat16

STEP = {"zl": 4, "zh": 12, "yl": 1, "yh": 3}
KV_ORDERS = (("zl", "zh", "yh"), ("zh", "yh", "zl"), ("yh", "zl", "zh"))
KV_ROWS = (192, 160, 160)
W_ORDERS = (
    ("zl", "yl", "zh", "yh"),
    ("yl", "zl", "yh", "zh"),
    ("zh", "yh", "zl", "yl"),
    ("yh", "zh", "yl", "zl"),
)


def patterns(order):
    found = [0]
    for name in order:
        found = found + [p ^ STEP[name] for p in found]
    return found


def chip_swap(array, flip, core_flip=0):
    pairs = [(j * 2 + c, (j ^ flip) * 2 + (c ^ core_flip)) for j in range(16) for c in range(2)]
    return lax.ppermute(array, "sp", pairs)


def core_swap(array):
    return chip_swap(array, 0, 1)


def shift_x(array, d):
    return lax.ppermute(array, "tp", [(i, (i + d) % 4) for i in range(4)])


def after(value, *others):
    return lax.optimization_barrier((value, others))[0]


def cost(us):
    return pl.CostEstimate(flops=int(us * 1e9), bytes_accessed=int(1e5), transcendentals=0)


def vmem_params(mib=48, **kw):
    return pltpu.CompilerParams(vmem_limit_bytes=mib << 20, **kw)


def flash_kernel(count, first, scale, *refs):
    q_ref, qpos_ref = refs[:2]
    kv_refs = refs[2 : 2 + count]
    kpos_refs = refs[2 + count : 2 + 2 * count]
    rest = refs[2 + 2 * count :]
    out_ref = rest[-1]
    rows = q_ref.shape[0]
    qpos = qpos_ref[...]
    state = []
    for s in range(2):
        if first:
            state.append(
                (jnp.full((rows, 1), NEG, F32), jnp.zeros((rows, 1), F32), jnp.zeros((rows, 256), F32))
            )
        else:
            st = rest[0]
            state.append(
                (st[:, 512 + s : 513 + s], st[:, 514 + s : 515 + s], st[:, 256 * s : 256 * s + 256])
            )
    for kv_ref, kpos_ref in zip(kv_refs, kpos_refs):
        visible = kpos_ref[...] <= qpos
        for s in range(2):
            top, total, acc = state[s]
            scores = lax.dot_general(
                q_ref[:, 128 * s : 128 * s + 128],
                kv_ref[:, 128 * s : 128 * s + 128],
                (((1,), (1,)), ((), ())),
                preferred_element_type=F32,
            )
            scores = jnp.where(visible, scores, NEG)
            new_top = jnp.maximum(top, jnp.max(scores, axis=1, keepdims=True))
            weights = jnp.exp2((scores - new_top) * scale)
            fade = jnp.exp2((top - new_top) * scale)
            total = total * fade + jnp.sum(weights, axis=1, keepdims=True)
            acc = acc * fade + jnp.dot(
                weights.astype(BF16), kv_ref[:, 256:512], preferred_element_type=F32
            )
            state[s] = (new_top, total, acc)
    lane = lax.broadcasted_iota(jnp.int32, (rows, 128), 1)
    tail = jnp.zeros((rows, 128), F32)
    for s in range(2):
        top, total, acc = state[s]
        out_ref[:, 256 * s : 256 * s + 256] = acc
        tail = jnp.where(lane == s, top, tail)
        tail = jnp.where(lane == 2 + s, total, tail)
    out_ref[:, 512:640] = tail


def flash(q, qpos, kvs, kposs, state, tile, us):
    rows = q.shape[0]
    scale = float(128**-0.5 * np.log2(np.e))
    row_block = lambda width: pl.BlockSpec((tile, width), lambda i: (i, 0))
    whole = lambda a: pl.BlockSpec(a.shape, lambda i: (0, 0))
    operands = [q, qpos, *kvs, *kposs] + ([] if state is None else [state])
    specs = [row_block(256), row_block(1)] + [whole(a) for a in (*kvs, *kposs)]
    if state is not None:
        specs.append(row_block(640))
    return pl.pallas_call(
        functools.partial(flash_kernel, len(kvs), state is None, scale),
        grid=(rows // tile,),
        in_specs=specs,
        out_specs=row_block(640),
        out_shape=jax.ShapeDtypeStruct((rows, 640), F32),
        compiler_params=vmem_params(),
        cost_estimate=cost(us),
        name="flash",
    )(*operands)


def merge_kernel(mine_ref, other_ref, lam_ref, gain_ref, out_ref):
    scale = float(128**-0.5 * np.log2(np.e))
    maps = []
    for s in range(2):
        top_a, top_b = mine_ref[:, 512 + s : 513 + s], other_ref[:, 512 + s : 513 + s]
        top = jnp.maximum(top_a, top_b)
        fade_a, fade_b = jnp.exp2((top_a - top) * scale), jnp.exp2((top_b - top) * scale)
        total = mine_ref[:, 514 + s : 515 + s] * fade_a + other_ref[:, 514 + s : 515 + s] * fade_b
        cols = slice(256 * s, 256 * s + 256)
        maps.append((mine_ref[:, cols] * fade_a + other_ref[:, cols] * fade_b) / total)
    contrast = maps[0] - lam_ref[...] * maps[1]
    power = jnp.mean(contrast * contrast, axis=-1, keepdims=True)
    out_ref[...] = (contrast * lax.rsqrt(power + EPS) * gain_ref[...]).astype(BF16)


def merge(mine, other, lam, gain):
    return pl.pallas_call(
        merge_kernel,
        grid=(2,),
        in_specs=[
            pl.BlockSpec((256, 640), lambda i: (i, 0)),
            pl.BlockSpec((256, 640), lambda i: (i, 0)),
            pl.BlockSpec((1, 256), lambda i: (0, 0)),
            pl.BlockSpec((1, 256), lambda i: (0, 0)),
        ],
        out_specs=pl.BlockSpec((256, 256), lambda i: (i, 0)),
        out_shape=jax.ShapeDtypeStruct((512, 256), BF16),
        compiler_params=vmem_params(),
        cost_estimate=cost(2),
        name="merge",
    )(mine, other, lam, gain)


def middle_kernel(*refs):
    blocks, weights = refs[0:4], refs[4:12]
    stream_ref, gain_ref, normed_ref, own_ref, scratch, power = refs[12:]
    step = pl.program_id(0)
    total = stream_ref[...].astype(F32)
    for d in range(4):
        block = blocks[d][...]
        if d:
            block = jnp.concatenate([block[64 * d :], block[: 64 * d]], axis=0)
        for half in range(2):
            total += jnp.dot(
                block[:, 256 * half : 256 * half + 256],
                weights[2 * d + half][...],
                preferred_element_type=F32,
            )
    squares = jnp.sum(total * total, axis=-1, keepdims=True)

    @pl.when(step == 0)
    def _():
        power[...] = jnp.broadcast_to(squares, power.shape)

    @pl.when(step > 0)
    def _():
        power[...] += jnp.broadcast_to(squares, power.shape)

    scratch[step] = total
    own_ref[...] = total[:64]

    @pl.when(step == 3)
    def _():
        root = lax.rsqrt(power[:, :1] * (1.0 / 2048) + EPS)
        for k in range(4):
            cols = slice(512 * k, 512 * k + 512)
            normed_ref[:, cols] = (scratch[k] * root * gain_ref[:, cols]).astype(BF16)


def middle_call(blocks, weights, stream, gain):
    return pl.pallas_call(
        middle_kernel,
        grid=(4,),
        in_specs=[pl.BlockSpec((256, 512), lambda i: (0, 0))] * 4
        + [pl.BlockSpec((256, 512), lambda i: (0, i))] * 8
        + [pl.BlockSpec((256, 512), lambda i: (0, i)), pl.BlockSpec((1, 2048), lambda i: (0, 0))],
        out_specs=[
            pl.BlockSpec((256, 2048), lambda i: (0, 0)),
            pl.BlockSpec((64, 512), lambda i: (0, i)),
        ],
        out_shape=[jax.ShapeDtypeStruct((256, 2048), BF16), jax.ShapeDtypeStruct((64, 2048), F32)],
        scratch_shapes=[pltpu.VMEM((4, 256, 512), F32), pltpu.VMEM((256, 128), F32)],
        compiler_params=vmem_params(),
        cost_estimate=cost(4),
        name="middle",
    )(*blocks, *weights, stream, gain)


def ffn_kernel(table, normed_ref, *refs):
    near, far_gu, far_d = refs[0:8], refs[8:16], refs[16:24]
    own_ref, *sent = refs[24:28]
    gu, down, hidden, sem = refs[28:]
    for side in range(2):
        for t in range(4):
            a, g, d = near[4 * side + t], far_gu[4 * side + t], far_d[4 * side + t]

            def body(i, _, a=a, g=g, d=d, side=side, t=t):
                base = (side * 4 + t) * 16
                first = pl.multiple_of(table[base + i], 16)
                second = pl.multiple_of(table[base + 8 + i], 16)
                pltpu.make_async_copy(
                    a.at[i, :, pl.ds(0, 2816)], gu.at[pl.ds(first, 16)], sem.at[0]
                ).start()
                pltpu.make_async_copy(g.at[i], gu.at[pl.ds(second, 16)], sem.at[0]).start()
                pltpu.make_async_copy(
                    a.at[i, :, pl.ds(2816, 1408)], down.at[pl.ds(first, 16)], sem.at[1]
                ).start()
                pltpu.make_async_copy(d.at[i], down.at[pl.ds(second, 16)], sem.at[1]).start()
                return 0

            lax.fori_loop(0, 8, body, 0)
    pltpu.make_async_copy(gu, gu, sem.at[0]).wait()

    def gate_up(k, _):
        cols = pl.ds(pl.multiple_of(k * 256, 256), 256)
        both = jnp.dot(normed_ref[...], gu[:, cols], preferred_element_type=F32)
        gate, up = both[:, :128], both[:, 128:]
        out = pl.ds(pl.multiple_of(k * 128, 128), 128)
        hidden[:, out] = (gate / (1.0 + jnp.exp(-gate)) * up).astype(BF16)
        return 0

    lax.fori_loop(0, 11, gate_up, 0)
    pltpu.make_async_copy(down, down, sem.at[1]).wait()

    def project(k, _):
        rows = pl.ds(pl.multiple_of(k * 256, 256), 256)
        part = lax.dot_general(
            hidden[...], down[rows, :], (((1,), (1,)), ((), ())), preferred_element_type=F32
        )
        own_ref[:, rows] = part[:64]
        for d in range(3):
            sent[d][:, rows] = part[64 * d + 64 : 64 * d + 128].astype(BF16)
        return 0

    lax.fori_loop(0, 8, project, 0)


def ffn(table, normed, near, far_gu, far_d):
    any_space = pl.BlockSpec(memory_space=pl.ANY)
    in_vmem = pl.BlockSpec(memory_space=pltpu.VMEM)
    return pl.pallas_call(
        ffn_kernel,
        in_specs=[pl.BlockSpec(memory_space=pltpu.SMEM), in_vmem] + [any_space] * 24,
        out_specs=[in_vmem] * 4,
        out_shape=[jax.ShapeDtypeStruct((64, 2048), F32)]
        + [jax.ShapeDtypeStruct((64, 2048), BF16)] * 3,
        scratch_shapes=[
            pltpu.VMEM((2048, 2816), BF16),
            pltpu.VMEM((2048, 1408), BF16),
            pltpu.VMEM((256, 1408), BF16),
            pltpu.SemaphoreType.DMA((2,)),
        ],
        compiler_params=vmem_params(),
        cost_estimate=cost(10),
        name="ffn",
    )(table, normed, *near, *far_gu, *far_d)


def shards(
    stream, queries, keys, values, head_lambda, head_gain, w_out, norm_gain, w_gate, w_up, w_down
):
    sp = lax.axis_index("sp")
    x = lax.axis_index("tp")
    core = sp % 2
    chip = sp // 2
    y = chip % 4
    second = jnp.logical_or(y == 1, y == 2)
    head = second.astype(jnp.int32)

    def own_head(array):
        return jnp.where(second, array[:, 256:], array[:, :256])

    def other_head(array):
        return jnp.where(second, array[:, :256], array[:, 256:])

    rolled = lax.dynamic_slice(jnp.concatenate([queries, queries]), (x * 64, 0), (256, 512))
    given = jnp.concatenate([other_head(keys), other_head(values), other_head(rolled)], axis=1)
    taken = chip_swap(given, STEP["yl"])
    kv = jnp.concatenate(
        [jnp.concatenate([own_head(keys), own_head(values)], axis=1), taken[:, :512]]
    )
    q_mine = jnp.concatenate([own_head(rolled), taken[:, 512:]])
    q_all = jnp.concatenate([q_mine, core_swap(q_mine)])

    def token(chip_of, core_of):
        return (chip_of * 2 + core_of) * 256

    in_roll = ((x + jnp.arange(256, dtype=jnp.int32) // 64) % 4) * 64 + jnp.arange(256) % 64
    qpos = jnp.concatenate(
        [
            token(chip ^ flip, core ^ core_flip) + in_roll
            for core_flip in (0, 1)
            for flip in (0, STEP["yl"])
        ]
    ).astype(jnp.int32)[:, None]

    kv_held, starts = [], [0, 192, 352]
    for t in range(3):
        kv_held.append(kv[starts[t] : starts[t] + KV_ROWS[t]][None])

    w_block = jnp.concatenate(
        [
            jnp.stack([w_gate.reshape(64, 11, 128), w_up.reshape(64, 11, 128)], axis=2).reshape(64, 2816),
            w_down.T,
        ],
        axis=1,
    ).reshape(4, 1, 16, 4224)
    w_held = [w_block[t] for t in range(4)]

    own_rows = (head ^ core) * 256
    w_mine = lax.dynamic_slice(w_out, (own_rows, 0), (256, 2048))
    w_other = lax.dynamic_slice(w_out, (256 - own_rows, 0), (256, 2048))

    kv_far = None
    gate = taken
    for s in range(3):
        kv_far = [chip_swap(kv_held[t], STEP[KV_ORDERS[t][s]]) for t in range(3)]
        if s < 2:
            kv_held = [jnp.concatenate([kv_held[t], kv_far[t]]) for t in range(3)]
        w_in = [after(w_held[t], *kv_far) for t in range(4)]
        w_far = [chip_swap(w_in[t], STEP[W_ORDERS[t][s]]) for t in range(4)]
        w_held = [jnp.concatenate([w_held[t], w_far[t]]) for t in range(4)]
        if s == 0:
            streams = [stream] + [shift_x(after(stream, *kv_far), d) for d in (1, 2, 3)]
            w_mines = [w_mine] + [shift_x(after(w_mine, *kv_far), d) for d in (1, 2, 3)]
    near_swapped = [core_swap(w) for w in w_held]
    far_gu = [chip_swap(w_held[t][:, :, :2816], STEP[W_ORDERS[t][3]]) for t in range(4)]
    far_d = [
        chip_swap(after(w_held[t][:, :, 2816:], *far_gu), STEP[W_ORDERS[t][3]]) for t in range(4)
    ]
    far_gu_swapped = [core_swap(w) for w in far_gu]
    far_d_swapped = [core_swap(w) for w in far_d]
    w_others = [w_other] + [core_swap(w) for w in w_mines[1:]]

    kpos_near, kpos_far = [], []
    for t in range(3):
        row = starts[t] + jnp.arange(KV_ROWS[t], dtype=jnp.int32)
        found = patterns(KV_ORDERS[t])
        pos = [
            token((chip ^ p) ^ (row >= 256).astype(jnp.int32), core) + row % 256 for p in found
        ]
        pos = [p.astype(jnp.int32) for p in pos]
        kpos_near.append(jnp.concatenate(pos[:4])[None])
        kpos_far.append(jnp.concatenate(pos[4:])[None])
    flat = lambda arrays: [a.reshape(-1, 512) for a in arrays]
    state = flash(q_all, qpos, flat(kv_held), kpos_near, None, 256, 6)
    sent = flash(q_all[512:], qpos[512:], flat(kv_far), kpos_far, state[512:], 256, 3)
    came = core_swap(sent)
    kept = flash(q_all[:512], qpos[:512], flat(kv_far), kpos_far, state[:512], 256, 3)
    lam = jnp.broadcast_to(jnp.where(second, head_lambda[1], head_lambda[0]), (1, 256))
    head_out = merge(kept, came, lam, head_gain[None])
    passed = chip_swap(head_out[256:], STEP["yl"])
    both = jnp.where(
        core == 0,
        jnp.concatenate([head_out[:256], passed], axis=1),
        jnp.concatenate([passed, head_out[:256]], axis=1),
    )
    blocks = [both] + [shift_x(both, d) for d in (1, 2, 3)]
    weights = [w for pair in zip(w_mines, w_others) for w in pair]
    rows = jnp.concatenate([streams[0], streams[3], streams[2], streams[1]])
    normed, middle = middle_call(blocks, weights, rows, norm_gain[None])

    table = []
    for side in range(2):
        for t in range(4):
            for p in patterns(W_ORDERS[t]):
                table.append(((chip ^ p) * 2 + (core ^ side)) * 64 + 16 * t)
    table = jnp.stack(table).astype(jnp.int32)
    own, *parts = ffn(
        table, normed, w_held + near_swapped, far_gu + far_gu_swapped, far_d + far_d_swapped
    )
    result = middle + own
    for d in (1, 2, 3):
        result = result + shift_x(parts[d - 1], d).astype(F32)
    return result.astype(BF16)


def solution(mesh):
    placed = (
        P(("sp", "tp"), None),
        P("sp", "tp"),
        P("sp", "tp"),
        P("sp", "tp"),
        P("tp"),
        P(),
        P("tp", None),
        P(),
        P("sp", "tp"),
        P("sp", "tp"),
        P("tp", "sp"),
    )
    return jax.shard_map(
        shards, mesh=mesh, in_specs=placed, out_specs=P(("sp", "tp"), None), check_vma=False
    )
```

```python
import functools

import jax
import jax.numpy as jnp
import numpy as np
from jax import lax
from jax.experimental import pallas as pl
from jax.experimental.pallas import tpu as pltpu
from jax.sharding import PartitionSpec as P


EPS = 1e-6
NEG = -1e30
F32 = jnp.float32
BF16 = jnp.bfloat16

STEP = {"zl": 4, "zh": 12, "yl": 1, "yh": 3}
KV_ORDERS = (("zl", "zh", "yh"), ("zh", "yh", "zl"), ("yh", "zl", "zh"))
KV_ROWS = (192, 160, 160)
KV_STARTS = (0, 96, 176)
W_ORDERS = (
    (("zl", "yl", "zh", "yh"), ("yl", "zl", "yh", "zh")),
    (("zh", "yh", "zl", "yl"), ("yh", "zh", "yl", "zl")),
)


def patterns(order):
    found = [0]
    for name in order:
        found = found + [p ^ STEP[name] for p in found]
    return found


def chip_swap(array, flip, core_flip=0):
    pairs = [(j * 2 + c, (j ^ flip) * 2 + (c ^ core_flip)) for j in range(16) for c in range(2)]
    return lax.ppermute(array, "sp", pairs)


def chip_swap_by_core(array, flips):
    pairs = [(j * 2 + c, (j ^ flips[c]) * 2 + c) for j in range(16) for c in range(2)]
    return lax.ppermute(array, "sp", pairs)


def core_swap(array):
    return chip_swap(array, 0, 1)


def shift_x(array, d):
    return lax.ppermute(array, "tp", [(i, (i + d) % 4) for i in range(4)])


def meta_layout():
    rows = [[(0, 0, 0, 0, 0)] * 2]
    for core_flip in (0, 1):
        rows.append([(0, 0, core_flip, 256, 0), (STEP["yl"],) * 2 + (core_flip, 256, 0)])
    for far in (0, 1):
        for t in range(3):
            for p in patterns(KV_ORDERS[t])[4 * far : 4 * far + 4]:
                rows.append(
                    [(p, p, 0, 256, KV_STARTS[t]), (p ^ STEP["yl"],) * 2 + (0, 256, KV_STARTS[t])]
                )
    for h in range(2):
        rows.append(
            [(a, b, h, 64, 0) for a, b in zip(patterns(W_ORDERS[0][h]), patterns(W_ORDERS[1][h]))]
        )
    return np.array([entry for row in rows for entry in row], np.int32)


META_Q, META_K, META_W = 2, 6, 54


def meta_table(head, x, chip, core):
    flip0, flip1, core_flip, factor, addend = (jnp.asarray(v) for v in meta_layout().T)
    flip = jnp.where(core == 0, flip0, flip1)
    table = ((chip ^ flip) * 2 + (core ^ core_flip)) * factor + addend
    place = jnp.arange(table.shape[0])
    table = jnp.where(place == 0, head, jnp.where(place == 1, x, table))
    return table.astype(jnp.int32)


def after(value, *others):
    return lax.optimization_barrier((value, others))[0]


def whole(shape):
    return pl.BlockSpec(shape, lambda *_: (0,) * len(shape))


def cost(us):
    return pl.CostEstimate(flops=int(us * 1e9), bytes_accessed=int(1e5), transcendentals=0)


def vmem_params(mib=24, **kw):
    return pltpu.CompilerParams(vmem_limit_bytes=mib << 20, **kw)


def pack_kernel(meta, keys, values, queries, own_ref, given_ref, ins, outs, sem):
    second, x = meta[0], meta[1]
    loads = [
        pltpu.make_async_copy(ref, ins.at[k], sem.at[k])
        for k, ref in enumerate((keys, values, queries))
    ]
    stores = [
        pltpu.make_async_copy(outs.at[k], ref, sem.at[3 + k])
        for k, ref in enumerate((given_ref, own_ref))
    ]
    for load in loads:
        load.start()
    for load in loads:
        load.wait()
    for k, turn in enumerate((1 - second, second)):
        cols = pl.ds(pl.multiple_of(turn * 256, 256), 256)
        outs[k, :, :256] = ins[0, :, cols]
        outs[k, :, 256:512] = ins[1, :, cols]
        for j in range(4):
            rows = pl.ds(pl.multiple_of(lax.rem(x + j, 4) * 64, 64), 64)
            outs[k, 64 * j : 64 * j + 64, 512:] = ins[2, rows, cols]
        stores[k].start()
    for store in stores:
        store.wait()


def pack(meta, keys, values, queries):
    in_hbm = pl.BlockSpec(memory_space=pltpu.HBM)
    return pl.pallas_call(
        pack_kernel,
        in_specs=[pl.BlockSpec(memory_space=pltpu.SMEM)] + [in_hbm] * 3,
        out_specs=[in_hbm] * 2,
        out_shape=[jax.ShapeDtypeStruct((256, 768), BF16)] * 2,
        scratch_shapes=[
            pltpu.VMEM((3, 256, 512), BF16),
            pltpu.VMEM((2, 256, 768), BF16),
            pltpu.SemaphoreType.DMA((5,)),
        ],
        compiler_params=vmem_params(16),
        cost_estimate=cost(1),
        name="pack",
    )(meta, keys, values, queries)


def weights_kernel(meta, gate, up, down, own_ref, given_ref):
    first = lax.rem(meta[META_Q] // 256, 2) == 0
    for k in range(2):
        cols = slice(704 * k, 704 * k + 704)
        block = jnp.concatenate(
            [gate[:, cols], up[:, cols], down[cols, :].T, jnp.zeros((64, 64), BF16)], axis=1
        )

        @pl.when(first == (k == 0))
        def _():
            own_ref[0] = block

        @pl.when(first != (k == 0))
        def _():
            given_ref[0] = block


def split_weights(meta, gate, up, down):
    return pl.pallas_call(
        weights_kernel,
        grid=(1,),
        in_specs=[pl.BlockSpec(memory_space=pltpu.SMEM)]
        + [whole((64, 1408))] * 2
        + [whole((1408, 64))],
        out_specs=[whole((1, 64, 2176))] * 2,
        out_shape=[jax.ShapeDtypeStruct((1, 64, 2176), BF16)] * 2,
        compiler_params=vmem_params(),
        cost_estimate=cost(2),
        name="weights",
    )(meta, gate, up, down)


def thirds_kernel(own, taken, *outs):
    for t in range(3):
        half, start = KV_ROWS[t] // 2, KV_STARTS[t]
        outs[t][0, :half] = own[start : start + half, :512]
        outs[t][0, half:] = taken[start : start + half, :512]
    outs[3][:256] = own[:, 512:]
    outs[3][256:] = taken[:, 512:]


def thirds(own, taken):
    shapes = [(1, n, 512) for n in KV_ROWS] + [(512, 256)]
    return pl.pallas_call(
        thirds_kernel,
        grid=(1,),
        in_specs=[whole((256, 768))] * 2,
        out_specs=[whole(shape) for shape in shapes],
        out_shape=[jax.ShapeDtypeStruct(shape, BF16) for shape in shapes],
        compiler_params=vmem_params(16),
        cost_estimate=cost(1),
        name="thirds",
    )(own, taken)


def join_kernel(count, *refs):
    for k in range(count):
        n = refs[k].shape[0]
        refs[2 * count + k][:n] = refs[k][...]
        refs[2 * count + k][n:] = refs[count + k][...]


def join(held, far):
    shapes = [(2 * a.shape[0], *a.shape[1:]) for a in held]
    return pl.pallas_call(
        functools.partial(join_kernel, len(held)),
        grid=(1,),
        in_specs=[whole(a.shape) for a in (*held, *far)],
        out_specs=[whole(shape) for shape in shapes],
        out_shape=[jax.ShapeDtypeStruct(shape, BF16) for shape in shapes],
        compiler_params=vmem_params(),
        cost_estimate=cost(1),
        name="join",
    )(*held, *far)


def flash_kernel(group, far, scale, meta, *refs):
    q_ref, kv_refs, rest = refs[0], refs[1:4], refs[4:]
    out_ref = rest[-1]
    step = pl.program_id(0)
    row = lax.broadcasted_iota(jnp.int32, (256, 1), 0)
    qpos = meta[META_Q + group + step] + ((meta[1] + (row >> 6)) & 3) * 64 + (row & 63)
    state = []
    for s in range(2):
        if far:
            st = rest[0]
            state.append(
                (st[:, 512 + s : 513 + s], st[:, 514 + s : 515 + s], st[:, 256 * s : 256 * s + 256])
            )
        else:
            state.append(
                (jnp.full((256, 1), NEG, F32), jnp.zeros((256, 1), F32), jnp.zeros((256, 256), F32))
            )
    for t in range(3):
        kv_ref, half = kv_refs[t], KV_ROWS[t] // 2
        key = lax.broadcasted_iota(jnp.int32, (1, 8 * half), 1)
        kpos = key
        for k in range(8):
            base = meta[META_K + 24 * far + 8 * t + k]
            kpos = jnp.where(key >= k * half, base + key - k * half, kpos)
        visible = kpos <= qpos
        for s in range(2):
            top, total, acc = state[s]
            scores = lax.dot_general(
                q_ref[:, 128 * s : 128 * s + 128],
                kv_ref[:, 128 * s : 128 * s + 128],
                (((1,), (1,)), ((), ())),
                preferred_element_type=F32,
            )
            scores = jnp.where(visible, scores, NEG)
            new_top = jnp.maximum(top, jnp.max(scores, axis=1, keepdims=True))
            weights = jnp.exp2((scores - new_top) * scale)
            fade = jnp.exp2((top - new_top) * scale)
            total = total * fade + jnp.sum(weights, axis=1, keepdims=True)
            acc = acc * fade + jnp.dot(
                weights.astype(BF16), kv_ref[:, 256:512], preferred_element_type=F32
            )
            state[s] = (new_top, total, acc)
    lane = lax.broadcasted_iota(jnp.int32, (256, 128), 1)
    tail = jnp.zeros((256, 128), F32)
    for s in range(2):
        top, total, acc = state[s]
        out_ref[:, 256 * s : 256 * s + 256] = acc
        tail = jnp.where(lane == s, top, tail)
        tail = jnp.where(lane == 2 + s, total, tail)
    out_ref[:, 512:640] = tail


def flash(meta, q, kvs, group, far, state, us):
    scale = float(128**-0.5 * np.log2(np.e))
    row_block = lambda width: pl.BlockSpec((256, width), lambda i: (i, 0))
    kvs = [a.reshape(-1, 512) for a in kvs]
    return pl.pallas_call(
        functools.partial(flash_kernel, group, far, scale),
        grid=(2,),
        in_specs=[pl.BlockSpec(memory_space=pltpu.SMEM), row_block(256)]
        + [pl.BlockSpec(a.shape, lambda i: (0, 0)) for a in kvs]
        + [row_block(640)] * far,
        out_specs=row_block(640),
        out_shape=jax.ShapeDtypeStruct((512, 640), F32),
        compiler_params=vmem_params(),
        cost_estimate=cost(us),
        name="flash",
    )(meta, q, *kvs, *([state] if far else []))


def merge_kernel(meta, lam, mine_ref, other_ref, gain_ref, out_ref):
    scale = float(128**-0.5 * np.log2(np.e))
    maps = []
    for s in range(2):
        top_a, top_b = mine_ref[:, 512 + s : 513 + s], other_ref[:, 512 + s : 513 + s]
        top = jnp.maximum(top_a, top_b)
        fade_a, fade_b = jnp.exp2((top_a - top) * scale), jnp.exp2((top_b - top) * scale)
        total = mine_ref[:, 514 + s : 515 + s] * fade_a + other_ref[:, 514 + s : 515 + s] * fade_b
        cols = slice(256 * s, 256 * s + 256)
        maps.append((mine_ref[:, cols] * fade_a + other_ref[:, cols] * fade_b) / total)
    contrast = maps[0] - lax.select(meta[0] == 1, lam[1], lam[0]) * maps[1]
    power = jnp.mean(contrast * contrast, axis=-1, keepdims=True)
    out_ref[0] = (contrast * lax.rsqrt(power + EPS) * gain_ref[...]).astype(BF16)


def merge(meta, lam, mine, other, gain):
    return pl.pallas_call(
        merge_kernel,
        grid=(2,),
        in_specs=[
            pl.BlockSpec(memory_space=pltpu.SMEM),
            pl.BlockSpec(memory_space=pltpu.SMEM),
            pl.BlockSpec((256, 640), lambda i: (i, 0)),
            pl.BlockSpec((256, 640), lambda i: (i, 0)),
            pl.BlockSpec((1, 256), lambda i: (0, 0)),
        ],
        out_specs=pl.BlockSpec((1, 256, 256), lambda i: (i, 0, 0)),
        out_shape=jax.ShapeDtypeStruct((2, 256, 256), BF16),
        compiler_params=vmem_params(),
        cost_estimate=cost(2),
        name="merge",
    )(meta, lam, mine, other, gain)


def middle_kernel(meta, *refs):
    owns, passes, weights, streams = refs[0:4], refs[4:8], refs[8:16], refs[16:20]
    gain_ref, normed_ref, own_ref, scratch, power = refs[20:]
    step = pl.program_id(0)
    total = jnp.concatenate([streams[d][...] for d in (0, 3, 2, 1)], axis=0).astype(F32)
    straight = (meta[META_Q] // 256) % 2 == 0
    for d in range(4):
        own, passed = owns[d][...], passes[d][...]
        for half in range(2):
            block = jnp.where(straight, *((own, passed) if half == 0 else (passed, own)))
            if d:
                block = jnp.concatenate([block[64 * d :], block[: 64 * d]], axis=0)
            total += jnp.dot(block, weights[2 * d + half][...], preferred_element_type=F32)
    squares = jnp.sum(total * total, axis=-1, keepdims=True)

    @pl.when(step == 0)
    def _():
        power[...] = jnp.broadcast_to(squares, power.shape)

    @pl.when(step > 0)
    def _():
        power[...] += jnp.broadcast_to(squares, power.shape)

    scratch[step] = total
    own_ref[...] = total[:64]

    @pl.when(step == 3)
    def _():
        root = lax.rsqrt(power[:, :1] * (1.0 / 2048) + EPS)
        for k in range(4):
            cols = slice(512 * k, 512 * k + 512)
            normed_ref[:, cols] = (scratch[k] * root * gain_ref[:, cols]).astype(BF16)


def middle_call(meta, owns, passes, weights, streams, gain):
    return pl.pallas_call(
        middle_kernel,
        grid=(4,),
        in_specs=[pl.BlockSpec(memory_space=pltpu.SMEM)]
        + [pl.BlockSpec((256, 256), lambda i: (0, 0))] * 8
        + [pl.BlockSpec((256, 512), lambda i: (0, i))] * 8
        + [pl.BlockSpec((64, 512), lambda i: (0, i))] * 4
        + [pl.BlockSpec((1, 2048), lambda i: (0, 0))],
        out_specs=[
            pl.BlockSpec((256, 2048), lambda i: (0, 0)),
            pl.BlockSpec((64, 512), lambda i: (0, i)),
        ],
        out_shape=[jax.ShapeDtypeStruct((256, 2048), BF16), jax.ShapeDtypeStruct((64, 2048), F32)],
        scratch_shapes=[pltpu.VMEM((4, 256, 512), F32), pltpu.VMEM((256, 128), F32)],
        compiler_params=vmem_params(),
        cost_estimate=cost(4),
        name="middle",
    )(meta, *owns, *passes, *weights, *streams, gain)


def ffn_kernel(table, mine_ref, other_ref, *refs):
    pieces = refs[:8]
    keep_ref, send_ref = refs[8:10]
    gu, down, both, hidden, sem = refs[10:]
    for k in range(8):

        def body(i, _, w=pieces[k], base=4 * k):
            row = pl.ds(pl.multiple_of(table[META_W + base + i], 64), 64)
            for n, (start, width) in enumerate(((0, 768), (768, 640))):
                pltpu.make_async_copy(
                    w.at[i, :, pl.ds(start, width)], gu.at[row, pl.ds(start, width)], sem.at[n]
                ).start()
            pltpu.make_async_copy(w.at[i, :, pl.ds(1408, 768)], down.at[row], sem.at[2]).start()
            return 0

        lax.fori_loop(0, 4, body, 0)

    def gate_up(cols):
        both[:256, cols] = jnp.dot(other_ref[...], gu[:, cols], preferred_element_type=F32)
        both[256:, cols] = jnp.dot(mine_ref[...], gu[:, cols], preferred_element_type=F32)

    def gate_up_pair(k, _):
        gate_up(pl.ds(pl.multiple_of(k * 256, 256), 256))
        return 0

    first, second = gu.at[:, pl.ds(0, 768)], gu.at[:, pl.ds(768, 640)]
    pltpu.make_async_copy(first, first, sem.at[0]).wait()
    lax.fori_loop(0, 3, gate_up_pair, 0)
    pltpu.make_async_copy(second, second, sem.at[1]).wait()
    lax.fori_loop(3, 5, gate_up_pair, 0)
    gate_up(pl.ds(1280, 128))

    def activate(k, _):
        rows = pl.ds(pl.multiple_of(k * 64, 64), 64)
        gate, up = both[rows, :704], both[rows, 704:]
        hidden[rows, :704] = (gate / (1.0 + jnp.exp(-gate)) * up).astype(BF16)
        hidden[rows, 704:] = jnp.zeros((64, 64), BF16)
        return 0

    lax.fori_loop(0, 8, activate, 0)
    pltpu.make_async_copy(down, down, sem.at[2]).wait()

    def project(k, _):
        rows = pl.ds(pl.multiple_of(k * 256, 256), 256)
        part = lax.dot_general(
            hidden[...], down[rows, :], (((1,), (1,)), ((), ())), preferred_element_type=F32
        )
        send_ref[:, rows] = part[:256].astype(BF16)
        keep_ref[:, rows] = part[256:]
        return 0

    lax.fori_loop(0, 8, project, 0)


def ffn(table, mine, other, pieces):
    any_space = pl.BlockSpec(memory_space=pl.ANY)
    in_vmem = pl.BlockSpec(memory_space=pltpu.VMEM)
    return pl.pallas_call(
        ffn_kernel,
        in_specs=[pl.BlockSpec(memory_space=pltpu.SMEM), in_vmem, in_vmem] + [any_space] * 8,
        out_specs=[in_vmem] * 2,
        out_shape=[jax.ShapeDtypeStruct((256, 2048), F32), jax.ShapeDtypeStruct((256, 2048), BF16)],
        scratch_shapes=[
            pltpu.VMEM((2048, 1408), BF16),
            pltpu.VMEM((2048, 768), BF16),
            pltpu.VMEM((512, 1408), F32),
            pltpu.VMEM((512, 768), BF16),
            pltpu.SemaphoreType.DMA((3,)),
        ],
        compiler_params=vmem_params(),
        cost_estimate=cost(9),
        name="ffn",
    )(table, mine, other, *pieces)


def add_kernel(mine_ref, came_ref, middle_ref, own_ref, *sent):
    total = mine_ref[...] + came_ref[...].astype(F32)
    own_ref[...] = total[:64] + middle_ref[...]
    for d in range(3):
        sent[d][...] = total[64 * d + 64 : 64 * d + 128].astype(BF16)


def add_parts(mine, came, middle):
    in_vmem = pl.BlockSpec(memory_space=pltpu.VMEM)
    return pl.pallas_call(
        add_kernel,
        in_specs=[in_vmem] * 3,
        out_specs=[in_vmem] * 4,
        out_shape=[jax.ShapeDtypeStruct((64, 2048), F32)]
        + [jax.ShapeDtypeStruct((64, 2048), BF16)] * 3,
        compiler_params=vmem_params(),
        cost_estimate=cost(1),
        name="add",
    )(mine, came, middle)


def layer(
    stream, queries, keys, values, head_lambda, head_gain, w_out, norm_gain, w_gate, w_up, w_down
):
    sp = lax.axis_index("sp")
    x = lax.axis_index("tp")
    core = sp % 2
    chip = sp // 2
    y = chip % 4
    second = jnp.logical_or(y == 1, y == 2)
    head = second.astype(jnp.int32)

    meta = meta_table(head, x, chip, core)
    own, given = pack(meta, keys, values, queries)
    *kv_held, q_mine = thirds(own, chip_swap(given, STEP["yl"]))
    q_other = core_swap(q_mine)

    w_own, w_given = split_weights(meta, w_gate, w_up, w_down)
    w_held = [w_own, core_swap(w_given)]

    own_rows = (head ^ core) * 256
    w_mine = lax.dynamic_slice(w_out, (own_rows, 0), (256, 2048))
    w_other = lax.dynamic_slice(w_out, (256 - own_rows, 0), (256, 2048))

    streams = [stream] + [shift_x(stream, d) for d in (1, 2, 3)]
    w_mines = [w_mine] + [shift_x(w_mine, d) for d in (1, 2, 3)]
    for s in range(3):
        kv_far = [chip_swap(kv_held[t], STEP[KV_ORDERS[t][s]]) for t in range(3)]
        if s < 2:
            kv_held = join(kv_held, kv_far)
        w_far = [
            chip_swap_by_core(w_held[h], [STEP[W_ORDERS[c][h][s]] for c in range(2)])
            for h in range(2)
        ]
        if s < 2:
            w_held = join(w_held, w_far)
    w_others = [w_other] + [core_swap(after(w, *kv_far)) for w in w_mines[1:]]

    state_other = flash(meta, q_other, kv_held, 2, 0, None, 5)
    state_mine = flash(meta, q_mine, kv_held, 0, 0, None, 5)
    last = [[STEP[W_ORDERS[c][h][3]] for c in range(2)] for h in range(2)]
    w_last = [chip_swap_by_core(after(w_held[h], *kv_far), last[h]) for h in range(2)]
    sent = flash(meta, q_other, kv_far, 2, 1, after(state_other, state_mine), 5)
    came = core_swap(sent)
    w_tail = [chip_swap_by_core(after(w_far[h], sent), last[h]) for h in range(2)]
    kept = flash(meta, q_mine, kv_far, 0, 1, state_mine, 5)
    head_out = merge(meta, head_lambda, kept, came, head_gain[None])
    mine_out, pair_out = head_out[0], head_out[1]
    passed = chip_swap(pair_out, STEP["yl"])
    owns = [mine_out] + [shift_x(mine_out, d) for d in (1, 2, 3)]
    passes = [passed] + [shift_x(passed, d) for d in (1, 2, 3)]

    weights = [w for pair in zip(w_mines, w_others) for w in pair]
    normed, middle = middle_call(meta, owns, passes, weights, streams, norm_gain[None])
    other_normed = core_swap(normed)
    kept_part, sent_part = ffn(
        meta,
        normed,
        other_normed,
        [w_held[0], w_far[0], w_last[0], w_tail[0], w_held[1], w_far[1], w_last[1], w_tail[1]],
    )
    result, *parts = add_parts(kept_part, core_swap(sent_part), middle)
    for d in (1, 2, 3):
        result = result + shift_x(parts[d - 1], d).astype(F32)
    return result.astype(BF16)


def solution(mesh):
    placed = (
        P(("sp", "tp"), None),
        P("sp", "tp"),
        P("sp", "tp"),
        P("sp", "tp"),
        P("tp"),
        P(),
        P("tp", None),
        P(),
        P("sp", "tp"),
        P("sp", "tp"),
        P("tp", "sp"),
    )
    return jax.shard_map(
        layer, mesh=mesh, in_specs=placed, out_specs=P(("sp", "tp"), None), check_vma=False
    )
```

```python
import functools

import jax
import jax.numpy as jnp
import numpy as np
from jax import lax
from jax.experimental import pallas as pl
from jax.experimental.pallas import tpu as pltpu
from jax.sharding import PartitionSpec as P


EPS = 1e-6
NEG = -1e30
F32 = jnp.float32
BF16 = jnp.bfloat16

STEP = {"zl": 4, "zh": 12, "yl": 1, "yh": 3}
KV_ORDERS = (("zl", "zh", "yh"), ("zh", "yh", "zl"), ("yh", "zl", "zh"))
KV_ROWS = (192, 160, 160)
KV_STARTS = (0, 96, 176)
W_ORDERS = (
    (("zl", "yl", "zh", "yh"), ("yl", "zl", "yh", "zh")),
    (("zh", "yh", "zl", "yl"), ("yh", "zh", "yl", "zl")),
)


def patterns(order):
    found = [0]
    for name in order:
        found = found + [p ^ STEP[name] for p in found]
    return found


def chip_swap(array, flip, core_flip=0):
    pairs = [(j * 2 + c, (j ^ flip) * 2 + (c ^ core_flip)) for j in range(16) for c in range(2)]
    return lax.ppermute(array, "sp", pairs)


def chip_swap_by_core(array, flips):
    pairs = [(j * 2 + c, (j ^ flips[c]) * 2 + c) for j in range(16) for c in range(2)]
    return lax.ppermute(array, "sp", pairs)


def core_swap(array):
    return chip_swap(array, 0, 1)


def shift_x(array, d):
    return lax.ppermute(array, "tp", [(i, (i + d) % 4) for i in range(4)])


def meta_layout():
    rows = [[(0, 0, 0, 0, 0)] * 2]
    for core_flip in (0, 1):
        rows.append([(0, 0, core_flip, 256, 0), (STEP["yl"],) * 2 + (core_flip, 256, 0)])
    for far in (0, 1):
        for t in range(3):
            for p in patterns(KV_ORDERS[t])[4 * far : 4 * far + 4]:
                rows.append(
                    [(p, p, 0, 256, KV_STARTS[t]), (p ^ STEP["yl"],) * 2 + (0, 256, KV_STARTS[t])]
                )
    for h in range(2):
        rows.append(
            [(a, b, h, 64, 0) for a, b in zip(patterns(W_ORDERS[0][h]), patterns(W_ORDERS[1][h]))]
        )
    return np.array([entry for row in rows for entry in row], np.int32)


META_Q, META_K, META_W = 2, 6, 54


def meta_table(head, x, chip, core):
    flip0, flip1, core_flip, factor, addend = (jnp.asarray(v) for v in meta_layout().T)
    flip = jnp.where(core == 0, flip0, flip1)
    table = ((chip ^ flip) * 2 + (core ^ core_flip)) * factor + addend
    place = jnp.arange(table.shape[0])
    table = jnp.where(place == 0, head, jnp.where(place == 1, x, table))
    return table.astype(jnp.int32)


def after(value, *others):
    return lax.optimization_barrier((value, others))[0]


def whole(shape):
    return pl.BlockSpec(shape, lambda *_: (0,) * len(shape))


def cost(us):
    return pl.CostEstimate(flops=int(us * 1e9), bytes_accessed=int(1e5), transcendentals=0)


def vmem_params(mib=16, **kw):
    return pltpu.CompilerParams(vmem_limit_bytes=mib << 20, **kw)


def pack_kernel(meta, keys, values, queries, own_ref, given_ref, ins, outs, sem):
    second, x = meta[0], meta[1]
    loads = [
        pltpu.make_async_copy(ref, ins.at[k], sem.at[k])
        for k, ref in enumerate((keys, values, queries))
    ]
    stores = [
        pltpu.make_async_copy(outs.at[k], ref, sem.at[3 + k])
        for k, ref in enumerate((given_ref, own_ref))
    ]
    for load in loads:
        load.start()
    for load in loads:
        load.wait()
    for k, turn in enumerate((1 - second, second)):
        cols = pl.ds(pl.multiple_of(turn * 256, 256), 256)
        outs[k, :, :256] = ins[0, :, cols]
        outs[k, :, 256:512] = ins[1, :, cols]
        for j in range(4):
            rows = pl.ds(pl.multiple_of(lax.rem(x + j, 4) * 64, 64), 64)
            outs[k, 64 * j : 64 * j + 64, 512:] = ins[2, rows, cols]
        stores[k].start()
    for store in stores:
        store.wait()


def pack(meta, keys, values, queries):
    in_hbm = pl.BlockSpec(memory_space=pltpu.HBM)
    return pl.pallas_call(
        pack_kernel,
        in_specs=[pl.BlockSpec(memory_space=pltpu.SMEM)] + [in_hbm] * 3,
        out_specs=[in_hbm] * 2,
        out_shape=[jax.ShapeDtypeStruct((256, 768), BF16)] * 2,
        scratch_shapes=[
            pltpu.VMEM((3, 256, 512), BF16),
            pltpu.VMEM((2, 256, 768), BF16),
            pltpu.SemaphoreType.DMA((5,)),
        ],
        compiler_params=vmem_params(63),
        cost_estimate=cost(1),
        name="pack",
    )(meta, keys, values, queries)


def weights_kernel(meta, gate, up, down, own_ref, given_ref):
    first = lax.rem(meta[META_Q] // 256, 2) == 0
    for k in range(2):
        cols = slice(704 * k, 704 * k + 704)
        block = jnp.concatenate(
            [gate[:, cols], up[:, cols], down[:, cols], jnp.zeros((64, 64), BF16)], axis=1
        )

        @pl.when(first == (k == 0))
        def _():
            own_ref[0] = block

        @pl.when(first != (k == 0))
        def _():
            given_ref[0] = block


def split_weights(meta, gate, up, down):
    return pl.pallas_call(
        weights_kernel,
        grid=(1,),
        in_specs=[pl.BlockSpec(memory_space=pltpu.SMEM)] + [whole((64, 1408))] * 3,
        out_specs=[whole((1, 64, 2176))] * 2,
        out_shape=[jax.ShapeDtypeStruct((1, 64, 2176), BF16)] * 2,
        compiler_params=vmem_params(63),
        cost_estimate=cost(2),
        name="weights",
    )(meta, gate, up, down)


def lines_kernel(meta, w_out, stream, out_ref, held, sem):
    half = pl.multiple_of((meta[0] ^ lax.rem(meta[META_Q] // 256, 2)) * 256, 256)
    loads = [
        pltpu.make_async_copy(w_out.at[pl.ds(half, 256)], held.at[pl.ds(0, 256)], sem.at[0]),
        pltpu.make_async_copy(stream, held.at[pl.ds(256, 64)], sem.at[1]),
    ]
    for load in loads:
        load.start()
    for load in loads:
        load.wait()
    store = pltpu.make_async_copy(held, out_ref, sem.at[2])
    store.start()
    store.wait()


def lines(meta, w_out, stream):
    in_hbm = pl.BlockSpec(memory_space=pltpu.HBM)
    return pl.pallas_call(
        lines_kernel,
        in_specs=[pl.BlockSpec(memory_space=pltpu.SMEM)] + [in_hbm] * 2,
        out_specs=in_hbm,
        out_shape=jax.ShapeDtypeStruct((320, 2048), BF16),
        scratch_shapes=[pltpu.VMEM((320, 2048), BF16), pltpu.SemaphoreType.DMA((3,))],
        compiler_params=vmem_params(63),
        cost_estimate=cost(2),
        name="lines",
    )(meta, w_out, stream)


def thirds_kernel(own, taken, *outs):
    for t in range(3):
        half, start = KV_ROWS[t] // 2, KV_STARTS[t]
        outs[t][0, :half] = own[start : start + half, :512]
        outs[t][0, half:] = taken[start : start + half, :512]
    outs[3][:256] = own[:, 512:]
    outs[3][256:] = taken[:, 512:]


def thirds(own, taken):
    shapes = [(1, n, 512) for n in KV_ROWS] + [(512, 256)]
    return pl.pallas_call(
        thirds_kernel,
        grid=(1,),
        in_specs=[whole((256, 768))] * 2,
        out_specs=[whole(shape) for shape in shapes],
        out_shape=[jax.ShapeDtypeStruct(shape, BF16) for shape in shapes],
        compiler_params=vmem_params(16),
        cost_estimate=cost(1),
        name="thirds",
    )(own, taken)


def join_kernel(count, *refs):
    for k in range(count):
        n = refs[k].shape[0]
        refs[2 * count + k][:n] = refs[k][...]
        refs[2 * count + k][n:] = refs[count + k][...]


def join(held, far):
    shapes = [(2 * a.shape[0], *a.shape[1:]) for a in held]
    return pl.pallas_call(
        functools.partial(join_kernel, len(held)),
        grid=(1,),
        in_specs=[whole(a.shape) for a in (*held, *far)],
        out_specs=[whole(shape) for shape in shapes],
        out_shape=[jax.ShapeDtypeStruct(shape, BF16) for shape in shapes],
        compiler_params=vmem_params(),
        cost_estimate=cost(1),
        name="join",
    )(*held, *far)


def flash_kernel(block, far, scale, meta, *refs):
    kv_refs, rest = refs[2:5], refs[5:]
    step = pl.program_id(0)
    row = lax.broadcasted_iota(jnp.int32, (256, 1), 0)
    qpos = (
        meta[META_Q + block + 2 * step] + ((meta[1] + (row >> 6)) & 3) * 64 + (row & 63)
    )
    queries = jnp.where(step == 0, refs[0][...], refs[1][...])
    state = []
    for _ in range(2):
        state.append(
            (jnp.full((256, 1), NEG, F32), jnp.zeros((256, 1), F32), jnp.zeros((256, 256), F32))
        )
    for t in range(3):
        kv_ref, half = kv_refs[t], KV_ROWS[t] // 2
        key = lax.broadcasted_iota(jnp.int32, (1, 8 * half), 1)
        kpos = key
        for k in range(8):
            base = meta[META_K + 24 * far + 8 * t + k]
            kpos = jnp.where(key >= k * half, base + key - k * half, kpos)
        visible = kpos <= qpos
        for s in range(2):
            top, total, acc = state[s]
            scores = lax.dot_general(
                queries[:, 128 * s : 128 * s + 128],
                kv_ref[:, 128 * s : 128 * s + 128],
                (((1,), (1,)), ((), ())),
                preferred_element_type=F32,
            )
            scores = jnp.where(visible, scores, NEG)
            new_top = jnp.maximum(top, jnp.max(scores, axis=1, keepdims=True))
            weights = jnp.exp2((scores - new_top) * scale)
            fade = jnp.exp2((top - new_top) * scale)
            total = total * fade + jnp.sum(weights, axis=1, keepdims=True)
            acc = acc * fade + jnp.dot(
                weights.astype(BF16), kv_ref[:, 256:512], preferred_element_type=F32
            )
            state[s] = (new_top, total, acc)
    lane = lax.broadcasted_iota(jnp.int32, (256, 128), 1)
    tail = jnp.zeros((256, 128), F32)
    for s in range(2):
        tail = jnp.where(lane == s, state[s][0], tail)
        tail = jnp.where(lane == 2 + s, state[s][1], tail)
    for k in range(2):

        @pl.when(step == k)
        def _():
            out_ref = rest[k - 2]
            if not far:
                for s in range(2):
                    out_ref[:, 256 * s : 256 * s + 256] = state[s][2]
                out_ref[:, 512:640] = tail
            else:
                near = rest[k]
                ends = jnp.zeros((256, 128), F32)
                for s in range(2):
                    top, total, acc = state[s]
                    near_top = near[:, 512 + s : 513 + s]
                    both_top = jnp.maximum(top, near_top)
                    fade = jnp.exp2((top - both_top) * scale)
                    near_fade = jnp.exp2((near_top - both_top) * scale)
                    total = total * fade + near[:, 514 + s : 515 + s] * near_fade
                    cols = slice(256 * s, 256 * s + 256)
                    out_ref[:, cols] = acc * fade + near[:, cols] * near_fade
                    ends = jnp.where(lane == s, both_top, ends)
                    ends = jnp.where(lane == 2 + s, total, ends)
                out_ref[:, 512:640] = ends


def flash(meta, block, q_mine, q_other, kvs, far, states, us):
    scale = float(128**-0.5 * np.log2(np.e))
    kvs = [a.reshape(-1, 512) for a in kvs]
    return pl.pallas_call(
        functools.partial(flash_kernel, block, far, scale),
        grid=(2,),
        in_specs=[pl.BlockSpec(memory_space=pltpu.SMEM)]
        + [pl.BlockSpec((256, 256), lambda i: (block, 0))] * 2
        + [whole(a.shape) for a in kvs]
        + [whole((256, 640))] * len(states),
        out_specs=[whole((256, 640))] * 2,
        out_shape=[jax.ShapeDtypeStruct((256, 640), F32)] * 2,
        compiler_params=vmem_params(),
        cost_estimate=cost(us),
        name="flash",
    )(meta, q_mine, q_other, *kvs, *states)


def merge_kernel(meta, lam, mine_ref, other_ref, gain_ref, out_ref):
    scale = float(128**-0.5 * np.log2(np.e))
    maps = []
    for s in range(2):
        top_a, top_b = mine_ref[:, 512 + s : 513 + s], other_ref[:, 512 + s : 513 + s]
        top = jnp.maximum(top_a, top_b)
        fade_a, fade_b = jnp.exp2((top_a - top) * scale), jnp.exp2((top_b - top) * scale)
        total = mine_ref[:, 514 + s : 515 + s] * fade_a + other_ref[:, 514 + s : 515 + s] * fade_b
        cols = slice(256 * s, 256 * s + 256)
        maps.append((mine_ref[:, cols] * fade_a + other_ref[:, cols] * fade_b) / total)
    contrast = maps[0] - lax.select(meta[0] == 1, lam[1], lam[0]) * maps[1]
    power = jnp.mean(contrast * contrast, axis=-1, keepdims=True)
    out_ref[...] = (contrast * lax.rsqrt(power + EPS) * gain_ref[...]).astype(BF16)


def merge(meta, lam, mine, other, gain):
    return pl.pallas_call(
        merge_kernel,
        grid=(1,),
        in_specs=[pl.BlockSpec(memory_space=pltpu.SMEM)] * 2
        + [whole((256, 640))] * 2
        + [whole((1, 256))],
        out_specs=whole((256, 256)),
        out_shape=jax.ShapeDtypeStruct((256, 256), BF16),
        compiler_params=vmem_params(),
        cost_estimate=cost(1),
        name="merge",
    )(meta, lam, mine, other, gain)


def merge_last_kernel(meta, lam, mine_ref, other_ref, gain_ref, passed_ref, out_ref, own):
    merge_kernel(meta, lam, mine_ref, other_ref, gain_ref, own)
    straight = lax.rem(meta[META_Q] // 256, 2) == 0
    out_ref[:, :256] = jnp.where(straight, own[...], passed_ref[...])
    out_ref[:, 256:] = jnp.where(straight, passed_ref[...], own[...])


def merge_last(meta, lam, mine, other, gain, passed):
    return pl.pallas_call(
        merge_last_kernel,
        grid=(1,),
        in_specs=[pl.BlockSpec(memory_space=pltpu.SMEM)] * 2
        + [whole((256, 640))] * 2
        + [whole((1, 256)), whole((256, 256))],
        out_specs=whole((256, 512)),
        out_shape=jax.ShapeDtypeStruct((256, 512), BF16),
        scratch_shapes=[pltpu.VMEM((256, 256), BF16)],
        compiler_params=vmem_params(),
        cost_estimate=cost(1),
        name="merge_last",
    )(meta, lam, mine, other, gain, passed)


def middle_kernel(meta, *refs):
    blocks, mines, others = refs[0:4], refs[4:8], refs[8:11]
    local, gain_ref, normed_ref, own_ref, scratch, power = refs[11:]
    step = pl.program_id(0)
    total = jnp.concatenate([mines[d][256:] for d in (0, 3, 2, 1)], axis=0).astype(F32)
    core = lax.rem(meta[META_Q] // 256, 2)
    rest = pl.ds(pl.multiple_of((1 - (meta[0] ^ core)) * 256, 256), 256)
    for d in range(4):
        rows = blocks[d][...]
        if d:
            rows = jnp.concatenate([rows[64 * d :], rows[: 64 * d]], axis=0)
        for half in range(2):
            block = rows[:, 256 * half : 256 * half + 256]
            if half == 0:
                weights = mines[d][:256]
            else:
                weights = others[d - 1][:256] if d else local[rest, :]
            total += jnp.dot(block, weights, preferred_element_type=F32)
    squares = jnp.sum(total * total, axis=-1, keepdims=True)

    @pl.when(step == 0)
    def _():
        power[...] = jnp.broadcast_to(squares, power.shape)

    @pl.when(step > 0)
    def _():
        power[...] += jnp.broadcast_to(squares, power.shape)

    scratch[step] = total
    own_ref[...] = total[:64]

    @pl.when(step == 3)
    def _():
        root = lax.rsqrt(power[:, :1] * (1.0 / 2048) + EPS)
        for k in range(4):
            cols = slice(512 * k, 512 * k + 512)
            normed_ref[:, cols] = (scratch[k] * root * gain_ref[:, cols]).astype(BF16)


def middle_call(meta, blocks, mines, others, w_out, gain):
    return pl.pallas_call(
        middle_kernel,
        grid=(4,),
        in_specs=[pl.BlockSpec(memory_space=pltpu.SMEM)]
        + [pl.BlockSpec((256, 512), lambda i: (0, 0))] * 4
        + [pl.BlockSpec((320, 512), lambda i: (0, i))] * 7
        + [pl.BlockSpec((512, 512), lambda i: (0, i))]
        + [pl.BlockSpec((1, 2048), lambda i: (0, 0))],
        out_specs=[
            pl.BlockSpec((256, 2048), lambda i: (0, 0)),
            pl.BlockSpec((64, 512), lambda i: (0, i)),
        ],
        out_shape=[jax.ShapeDtypeStruct((256, 2048), BF16), jax.ShapeDtypeStruct((64, 2048), F32)],
        scratch_shapes=[pltpu.VMEM((4, 256, 512), F32), pltpu.VMEM((256, 128), F32)],
        compiler_params=vmem_params(),
        cost_estimate=cost(4),
        name="middle",
    )(meta, *blocks, *mines, *others, w_out, gain)


def ffn_kernel(table, mine_ref, other_ref, *refs):
    pieces = refs[:8]
    keep_ref, send_ref = refs[8:10]
    gu, down, both, hidden, sem = refs[10:]
    for k in range(8):

        def body(i, _, w=pieces[k], base=4 * k):
            row = pl.ds(pl.multiple_of(table[META_W + base + i], 64), 64)
            for n, (start, width) in enumerate(((0, 768), (768, 640))):
                pltpu.make_async_copy(
                    w.at[i, :, pl.ds(start, width)], gu.at[row, pl.ds(start, width)], sem.at[n]
                ).start()
            pltpu.make_async_copy(w.at[i, :, pl.ds(1408, 768)], down.at[row], sem.at[2]).start()
            return 0

        lax.fori_loop(0, 4, body, 0)

    def gate_up(cols):
        both[:256, cols] = jnp.dot(other_ref[...], gu[:, cols], preferred_element_type=F32)
        both[256:, cols] = jnp.dot(mine_ref[...], gu[:, cols], preferred_element_type=F32)

    first, second = gu.at[:, pl.ds(0, 768)], gu.at[:, pl.ds(768, 640)]
    pltpu.make_async_copy(first, first, sem.at[0]).wait()
    gate_up(pl.ds(0, 768))
    pltpu.make_async_copy(second, second, sem.at[1]).wait()
    gate_up(pl.ds(768, 640))

    def activate(k, _):
        rows = pl.ds(pl.multiple_of(k * 128, 128), 128)
        gate, up = both[rows, :704], both[rows, 704:]
        hidden[rows, :704] = (gate / (1.0 + jnp.exp(-gate)) * up).astype(BF16)
        hidden[rows, 704:] = jnp.zeros((128, 64), BF16)
        return 0

    lax.fori_loop(0, 4, activate, 0)
    pltpu.make_async_copy(down, down, sem.at[2]).wait()

    def project(k, _):
        rows = pl.ds(pl.multiple_of(k * 512, 512), 512)
        part = lax.dot_general(
            hidden[...], down[rows, :], (((1,), (1,)), ((), ())), preferred_element_type=F32
        )
        send_ref[:, rows] = part[:256].astype(BF16)
        keep_ref[:, rows] = part[256:]
        return 0

    lax.fori_loop(0, 4, project, 0)


def ffn(table, mine, other, pieces):
    any_space = pl.BlockSpec(memory_space=pl.ANY)
    in_vmem = pl.BlockSpec(memory_space=pltpu.VMEM)
    return pl.pallas_call(
        ffn_kernel,
        in_specs=[pl.BlockSpec(memory_space=pltpu.SMEM), in_vmem, in_vmem] + [any_space] * 8,
        out_specs=[in_vmem] * 2,
        out_shape=[jax.ShapeDtypeStruct((256, 2048), F32), jax.ShapeDtypeStruct((256, 2048), BF16)],
        scratch_shapes=[
            pltpu.VMEM((2048, 1408), BF16),
            pltpu.VMEM((2048, 768), BF16),
            pltpu.VMEM((512, 1408), F32),
            pltpu.VMEM((512, 768), BF16),
            pltpu.SemaphoreType.DMA((3,)),
        ],
        compiler_params=vmem_params(28),
        cost_estimate=cost(9),
        name="ffn",
    )(table, mine, other, *pieces)


def add_kernel(mine_ref, came_ref, middle_ref, own_ref, *sent):
    total = mine_ref[...] + came_ref[...].astype(F32)
    own_ref[...] = total[:64] + middle_ref[...]
    for d in range(3):
        sent[d][...] = total[64 * d + 64 : 64 * d + 128].astype(BF16)


def add_parts(mine, came, middle):
    in_vmem = pl.BlockSpec(memory_space=pltpu.VMEM)
    return pl.pallas_call(
        add_kernel,
        in_specs=[in_vmem] * 3,
        out_specs=[in_vmem] * 4,
        out_shape=[jax.ShapeDtypeStruct((64, 2048), F32)]
        + [jax.ShapeDtypeStruct((64, 2048), BF16)] * 3,
        compiler_params=vmem_params(),
        cost_estimate=cost(1),
        name="add",
    )(mine, came, middle)


def layer(
    stream, queries, keys, values, head_lambda, head_gain, w_out, norm_gain, w_gate, w_up, w_down
):
    sp = lax.axis_index("sp")
    x = lax.axis_index("tp")
    core = sp % 2
    chip = sp // 2
    y = chip % 4
    second = jnp.logical_or(y == 1, y == 2)
    head = second.astype(jnp.int32)

    meta = meta_table(head, x, chip, core)
    own, given = pack(meta, keys, values, queries)
    *kv_held, q_mine = thirds(own, chip_swap(given, STEP["yl"]))
    q_other = core_swap(q_mine)

    w_own, w_given = split_weights(meta, w_gate, w_up, w_down.T)
    w_held = [w_own, core_swap(w_given)]

    line = lines(meta, w_out, stream)
    w_mines = [line] + [shift_x(line, d) for d in (1, 2, 3)]
    for s in range(3):
        kv_far = [chip_swap(kv_held[t], STEP[KV_ORDERS[t][s]]) for t in range(3)]
        if s < 2:
            kv_held = join(kv_held, kv_far)
    states_p = flash(meta, 1, q_mine, q_other, kv_held, 0, [], 5)
    states_o = flash(meta, 0, after(q_mine, *states_p), q_other, kv_held, 0, [], 5)

    def w_step(s, h, array):
        return chip_swap_by_core(array, [STEP[W_ORDERS[c][h][s]] for c in range(2)])

    w_far = [w_step(0, h, w_held[h]) for h in range(2)]
    w_held = join(w_held, w_far)
    w_far = [w_step(1, h, after(w_held[h], *states_p)) for h in range(2)]

    kept, sent = flash(meta, 1, after(q_mine, *states_o), q_other, kv_far, 1, states_p, 5)
    came = core_swap(sent)
    w_held = join([after(w, sent) for w in w_held], w_far)
    w_far = [w_step(2, h, w_held[h]) for h in range(2)]
    w_last1 = w_step(3, 1, w_held[1])
    pair_out = merge(meta, head_lambda, kept, came, head_gain[None])
    passed = chip_swap(pair_out, STEP["yl"])
    w_last0 = w_step(3, 0, after(w_held[0], pair_out))
    kept, sent = flash(meta, 0, after(q_mine, pair_out), q_other, kv_far, 1, states_o, 5)
    came = core_swap(sent)
    block = merge_last(meta, head_lambda, kept, came, head_gain[None], passed)
    blocks = [block] + [shift_x(block, d) for d in (1, 2, 3)]
    w_others = [core_swap(after(w, block)) for w in w_mines[1:]]
    w_tail = [w_step(3, h, after(w_far[h], block)) for h in range(2)]
    w_last = [w_last0, w_last1]
    normed, middle = middle_call(meta, blocks, w_mines, w_others, w_out, norm_gain[None])
    other_normed = core_swap(normed)
    kept_part, sent_part = ffn(
        meta,
        normed,
        other_normed,
        [w_held[0], w_far[0], w_last[0], w_tail[0], w_held[1], w_far[1], w_last[1], w_tail[1]],
    )
    result, *parts = add_parts(kept_part, core_swap(sent_part), middle)
    for d in (1, 2, 3):
        result = result + shift_x(parts[d - 1], d).astype(F32)
    return result.astype(BF16)


def solution(mesh):
    placed = (
        P(("sp", "tp"), None),
        P("sp", "tp"),
        P("sp", "tp"),
        P("sp", "tp"),
        P("tp"),
        P(),
        P("tp", None),
        P(),
        P("sp", "tp"),
        P("sp", "tp"),
        P("tp", "sp"),
    )
    return jax.shard_map(
        layer, mesh=mesh, in_specs=placed, out_specs=P(("sp", "tp"), None), check_vma=False
    )
```

```python
import functools

import jax
import jax.numpy as jnp
import numpy as np
from jax import lax
from jax.experimental import pallas as pl
from jax.experimental.pallas import tpu as pltpu
from jax.sharding import PartitionSpec as P


EPS = 1e-6
NEG = -1e30
F32 = jnp.float32
BF16 = jnp.bfloat16

STEP = {"zl": 4, "zh": 12, "yl": 1, "yh": 3}
KV_ORDERS = (("zl", "zh", "yh"), ("zh", "yh", "zl"), ("yh", "zl", "zh"))
KV_ROWS = (192, 160, 160)
KV_STARTS = (0, 96, 176)
W_ORDERS = (
    (("zl", "yl", "zh", "yh"), ("yl", "zl", "yh", "zh")),
    (("zh", "yh", "zl", "yl"), ("yh", "zh", "yl", "zl")),
)


def patterns(order):
    found = [0]
    for name in order:
        found = found + [p ^ STEP[name] for p in found]
    return found


def chip_swap(array, flip, core_flip=0):
    pairs = [(j * 2 + c, (j ^ flip) * 2 + (c ^ core_flip)) for j in range(16) for c in range(2)]
    return lax.ppermute(array, "sp", pairs)


def chip_swap_by_core(array, flips):
    pairs = [(j * 2 + c, (j ^ flips[c]) * 2 + c) for j in range(16) for c in range(2)]
    return lax.ppermute(array, "sp", pairs)


def core_swap(array):
    return chip_swap(array, 0, 1)


def shift_x(array, d):
    return lax.ppermute(array, "tp", [(i, (i + d) % 4) for i in range(4)])


def meta_layout():
    rows = [[(0, 0, 0, 0, 0)] * 2]
    for core_flip in (0, 1):
        rows.append([(0, 0, core_flip, 256, 0), (STEP["yl"],) * 2 + (core_flip, 256, 0)])
    for far in (0, 1):
        for t in range(3):
            for p in patterns(KV_ORDERS[t])[4 * far : 4 * far + 4]:
                rows.append(
                    [(p, p, 0, 256, KV_STARTS[t]), (p ^ STEP["yl"],) * 2 + (0, 256, KV_STARTS[t])]
                )
    for h in range(2):
        rows.append(
            [(a, b, h, 64, 0) for a, b in zip(patterns(W_ORDERS[0][h]), patterns(W_ORDERS[1][h]))]
        )
    return np.array([entry for row in rows for entry in row], np.int32)


META_Q, META_K, META_W = 2, 6, 54


def meta_table(head, x, chip, core):
    flip0, flip1, core_flip, factor, addend = (jnp.asarray(v) for v in meta_layout().T)
    flip = jnp.where(core == 0, flip0, flip1)
    table = ((chip ^ flip) * 2 + (core ^ core_flip)) * factor + addend
    place = jnp.arange(table.shape[0])
    table = jnp.where(place == 0, head, jnp.where(place == 1, x, table))
    return table.astype(jnp.int32)


def after(value, *others):
    return lax.optimization_barrier((value, others))[0]


def whole(shape):
    return pl.BlockSpec(shape, lambda *_: (0,) * len(shape))


def cost(us):
    return pl.CostEstimate(flops=int(us * 1e9), bytes_accessed=int(1e5), transcendentals=0)


def vmem_params(mib=16, **kw):
    return pltpu.CompilerParams(vmem_limit_bytes=mib << 20, **kw)


def pack_kernel(keys, values, queries, own_ref, given_ref, ins, outs, sem):
    y, x = lax.rem(lax.axis_index("sp") // 2, 4), lax.axis_index("tp")
    second = jnp.where((y == 1) | (y == 2), 1, 0)
    loads = [
        pltpu.make_async_copy(ref, ins.at[k], sem.at[k])
        for k, ref in enumerate((keys, values, queries))
    ]
    stores = [
        pltpu.make_async_copy(outs.at[k], ref, sem.at[3 + k])
        for k, ref in enumerate((given_ref, own_ref))
    ]
    for load in loads:
        load.start()
    for load in loads:
        load.wait()
    for k, turn in enumerate((1 - second, second)):
        cols = pl.ds(pl.multiple_of(turn * 256, 256), 256)
        outs[k, :, :256] = ins[0, :, cols]
        outs[k, :, 256:512] = ins[1, :, cols]
        for j in range(4):
            rows = pl.ds(pl.multiple_of(lax.rem(x + j, 4) * 64, 64), 64)
            outs[k, 64 * j : 64 * j + 64, 512:] = ins[2, rows, cols]
        stores[k].start()
    for store in stores:
        store.wait()


def pack(keys, values, queries):
    in_hbm = pl.BlockSpec(memory_space=pltpu.HBM)
    return pl.pallas_call(
        pack_kernel,
        in_specs=[in_hbm] * 3,
        out_specs=[in_hbm] * 2,
        out_shape=[jax.ShapeDtypeStruct((256, 768), BF16)] * 2,
        scratch_shapes=[
            pltpu.VMEM((3, 256, 512), BF16),
            pltpu.VMEM((2, 256, 768), BF16),
            pltpu.SemaphoreType.DMA((5,)),
        ],
        compiler_params=vmem_params(63),
        cost_estimate=cost(1),
        name="pack",
    )(keys, values, queries)


def weights_kernel(meta, gate, up, down, own_ref, given_ref):
    first = lax.rem(meta[META_Q] // 256, 2) == 0
    for k in range(2):
        cols = slice(704 * k, 704 * k + 704)
        block = jnp.concatenate(
            [gate[:, cols], up[:, cols], down[:, cols], jnp.zeros((64, 64), BF16)], axis=1
        )

        @pl.when(first == (k == 0))
        def _():
            own_ref[0] = block

        @pl.when(first != (k == 0))
        def _():
            given_ref[0] = block


def split_weights(meta, gate, up, down):
    return pl.pallas_call(
        weights_kernel,
        grid=(1,),
        in_specs=[pl.BlockSpec(memory_space=pltpu.SMEM)] + [whole((64, 1408))] * 3,
        out_specs=[whole((1, 64, 2176))] * 2,
        out_shape=[jax.ShapeDtypeStruct((1, 64, 2176), BF16)] * 2,
        compiler_params=vmem_params(63),
        cost_estimate=cost(2),
        name="weights",
    )(meta, gate, up, down)


def lines_kernel(meta, w_out, stream, out_ref, held, sem):
    half = pl.multiple_of((meta[0] ^ lax.rem(meta[META_Q] // 256, 2)) * 256, 256)
    loads = [
        pltpu.make_async_copy(w_out.at[pl.ds(half, 256)], held.at[pl.ds(0, 256)], sem.at[0]),
        pltpu.make_async_copy(stream, held.at[pl.ds(256, 64)], sem.at[1]),
    ]
    for load in loads:
        load.start()
    for load in loads:
        load.wait()
    store = pltpu.make_async_copy(held, out_ref, sem.at[2])
    store.start()
    store.wait()


def lines(meta, w_out, stream):
    in_hbm = pl.BlockSpec(memory_space=pltpu.HBM)
    return pl.pallas_call(
        lines_kernel,
        in_specs=[pl.BlockSpec(memory_space=pltpu.SMEM)] + [in_hbm] * 2,
        out_specs=in_hbm,
        out_shape=jax.ShapeDtypeStruct((320, 2048), BF16),
        scratch_shapes=[pltpu.VMEM((320, 2048), BF16), pltpu.SemaphoreType.DMA((3,))],
        compiler_params=vmem_params(63),
        cost_estimate=cost(2),
        name="lines",
    )(meta, w_out, stream)


def thirds_kernel(own, taken, *outs):
    for t in range(3):
        half, start = KV_ROWS[t] // 2, KV_STARTS[t]
        outs[t][0, :half] = own[start : start + half, :512]
        outs[t][0, half:] = taken[start : start + half, :512]
    outs[3][:256] = own[:, 512:]
    outs[3][256:] = taken[:, 512:]


def thirds(own, taken):
    shapes = [(1, n, 512) for n in KV_ROWS] + [(512, 256)]
    return pl.pallas_call(
        thirds_kernel,
        grid=(1,),
        in_specs=[whole((256, 768))] * 2,
        out_specs=[whole(shape) for shape in shapes],
        out_shape=[jax.ShapeDtypeStruct(shape, BF16) for shape in shapes],
        compiler_params=vmem_params(16),
        cost_estimate=cost(1),
        name="thirds",
    )(own, taken)


def join_kernel(count, *refs):
    for k in range(count):
        n = refs[k].shape[0]
        refs[2 * count + k][:n] = refs[k][...]
        refs[2 * count + k][n:] = refs[count + k][...]


def join(held, far):
    shapes = [(2 * a.shape[0], *a.shape[1:]) for a in held]
    return pl.pallas_call(
        functools.partial(join_kernel, len(held)),
        grid=(1,),
        in_specs=[whole(a.shape) for a in (*held, *far)],
        out_specs=[whole(shape) for shape in shapes],
        out_shape=[jax.ShapeDtypeStruct(shape, BF16) for shape in shapes],
        compiler_params=vmem_params(),
        cost_estimate=cost(1),
        name="join",
    )(*held, *far)


def flash_first_kernel(block, scale, meta, *refs):
    kv_refs, rest = refs[2:5], refs[5:]
    row = lax.broadcasted_iota(jnp.int32, (512, 1), 0)
    qpos = (
        jnp.where(row < 256, meta[META_Q + block], meta[META_Q + block + 2])
        + ((meta[1] + (row >> 6)) & 3) * 64
        + (row & 63)
    )
    queries = jnp.concatenate([refs[0][...], refs[1][...]], axis=0)
    state = []
    for _ in range(2):
        state.append(
            (jnp.full((512, 1), NEG, F32), jnp.zeros((512, 1), F32), jnp.zeros((512, 256), F32))
        )
    for t in range(3):
        kv_ref, half = kv_refs[t], KV_ROWS[t] // 2
        key = lax.broadcasted_iota(jnp.int32, (1, 8 * half), 1)
        kpos = key
        for k in range(8):
            base = meta[META_K + 8 * t + k]
            kpos = jnp.where(key >= k * half, base + key - k * half, kpos)
        visible = kpos <= qpos
        for s in range(2):
            top, total, acc = state[s]
            scores = lax.dot_general(
                queries[:, 128 * s : 128 * s + 128],
                kv_ref[:, 128 * s : 128 * s + 128],
                (((1,), (1,)), ((), ())),
                preferred_element_type=F32,
            )
            scores = jnp.where(visible, scores, NEG)
            new_top = jnp.maximum(top, jnp.max(scores, axis=1, keepdims=True))
            weights = jnp.exp2((scores - new_top) * scale)
            fade = jnp.exp2((top - new_top) * scale)
            total = total * fade + jnp.sum(weights, axis=1, keepdims=True)
            acc = acc * fade + jnp.dot(
                weights.astype(BF16), kv_ref[:, 256:512], preferred_element_type=F32
            )
            state[s] = (new_top, total, acc)
    lane = lax.broadcasted_iota(jnp.int32, (256, 128), 1)
    for k in range(2):
        out_ref = rest[k - 2]
        rows = slice(256 * k, 256 * k + 256)
        tail = jnp.zeros((256, 128), F32)
        for s in range(2):
            top, total, acc = (part[rows] for part in state[s])
            cols = slice(256 * s, 256 * s + 256)
            out_ref[:, cols] = acc
            tail = jnp.where(lane == s, top, tail)
            tail = jnp.where(lane == 2 + s, total, tail)
        out_ref[:, 512:640] = tail


def flash_last_kernel(block, scale, meta, *refs):
    kv_refs, rest = refs[2:5], refs[5:]
    step = pl.program_id(0)
    row = lax.broadcasted_iota(jnp.int32, (256, 1), 0)
    qpos = (
        meta[META_Q + block + 2 * step] + ((meta[1] + (row >> 6)) & 3) * 64 + (row & 63)
    )
    queries = jnp.where(step == 0, refs[0][...], refs[1][...])
    state = []
    for _ in range(2):
        state.append(
            (jnp.full((256, 1), NEG, F32), jnp.zeros((256, 1), F32), jnp.zeros((256, 256), F32))
        )
    for t in range(3):
        kv_ref, half = kv_refs[t], KV_ROWS[t] // 2
        key = lax.broadcasted_iota(jnp.int32, (1, 8 * half), 1)
        kpos = key
        for k in range(8):
            base = meta[META_K + 24 + 8 * t + k]
            kpos = jnp.where(key >= k * half, base + key - k * half, kpos)
        visible = kpos <= qpos
        for s in range(2):
            top, total, acc = state[s]
            scores = lax.dot_general(
                queries[:, 128 * s : 128 * s + 128],
                kv_ref[:, 128 * s : 128 * s + 128],
                (((1,), (1,)), ((), ())),
                preferred_element_type=F32,
            )
            scores = jnp.where(visible, scores, NEG)
            new_top = jnp.maximum(top, jnp.max(scores, axis=1, keepdims=True))
            weights = jnp.exp2((scores - new_top) * scale)
            fade = jnp.exp2((top - new_top) * scale)
            total = total * fade + jnp.sum(weights, axis=1, keepdims=True)
            acc = acc * fade + jnp.dot(
                weights.astype(BF16), kv_ref[:, 256:512], preferred_element_type=F32
            )
            state[s] = (new_top, total, acc)
    lane = lax.broadcasted_iota(jnp.int32, (256, 128), 1)
    for k in range(2):

        @pl.when(step == k)
        def _():
            out_ref = rest[k - 2]
            near = rest[k]
            ends = jnp.zeros((256, 128), F32)
            for s in range(2):
                top, total, acc = state[s]
                near_top = near[:, 512 + s : 513 + s]
                both_top = jnp.maximum(top, near_top)
                fade = jnp.exp2((top - both_top) * scale)
                near_fade = jnp.exp2((near_top - both_top) * scale)
                total = total * fade + near[:, 514 + s : 515 + s] * near_fade
                cols = slice(256 * s, 256 * s + 256)
                out_ref[:, cols] = acc * fade + near[:, cols] * near_fade
                ends = jnp.where(lane == s, both_top, ends)
                ends = jnp.where(lane == 2 + s, total, ends)
            out_ref[:, 512:640] = ends


def flash(meta, block, q_mine, q_other, kvs, states, us):
    scale = float(128**-0.5 * np.log2(np.e))
    kvs = [a.reshape(-1, 512) for a in kvs]
    return pl.pallas_call(
        functools.partial(flash_last_kernel if states else flash_first_kernel, block, scale),
        grid=(2,) if states else (1,),
        in_specs=[pl.BlockSpec(memory_space=pltpu.SMEM)]
        + [pl.BlockSpec((256, 256), lambda i: (block, 0))] * 2
        + [whole(a.shape) for a in kvs]
        + [whole((256, 640))] * len(states),
        out_specs=[whole((256, 640))] * 2,
        out_shape=[jax.ShapeDtypeStruct((256, 640), F32)] * 2,
        compiler_params=vmem_params(),
        cost_estimate=cost(us),
        name="flash",
    )(meta, q_mine, q_other, *kvs, *states)


def merge_kernel(meta, lam, mine_ref, other_ref, gain_ref, out_ref):
    scale = float(128**-0.5 * np.log2(np.e))
    maps = []
    for s in range(2):
        top_a, top_b = mine_ref[:, 512 + s : 513 + s], other_ref[:, 512 + s : 513 + s]
        top = jnp.maximum(top_a, top_b)
        fade_a, fade_b = jnp.exp2((top_a - top) * scale), jnp.exp2((top_b - top) * scale)
        total = mine_ref[:, 514 + s : 515 + s] * fade_a + other_ref[:, 514 + s : 515 + s] * fade_b
        cols = slice(256 * s, 256 * s + 256)
        maps.append((mine_ref[:, cols] * fade_a + other_ref[:, cols] * fade_b) / total)
    contrast = maps[0] - lax.select(meta[0] == 1, lam[1], lam[0]) * maps[1]
    power = jnp.mean(contrast * contrast, axis=-1, keepdims=True)
    out_ref[...] = (contrast * lax.rsqrt(power + EPS) * gain_ref[...]).astype(BF16)


def merge(meta, lam, mine, other, gain):
    return pl.pallas_call(
        merge_kernel,
        grid=(1,),
        in_specs=[pl.BlockSpec(memory_space=pltpu.SMEM)] * 2
        + [whole((256, 640))] * 2
        + [whole((1, 256))],
        out_specs=whole((256, 256)),
        out_shape=jax.ShapeDtypeStruct((256, 256), BF16),
        compiler_params=vmem_params(),
        cost_estimate=cost(1),
        name="merge",
    )(meta, lam, mine, other, gain)


def merge_last_kernel(meta, lam, mine_ref, other_ref, gain_ref, passed_ref, out_ref, own):
    merge_kernel(meta, lam, mine_ref, other_ref, gain_ref, own)
    straight = lax.rem(meta[META_Q] // 256, 2) == 0
    out_ref[:, :256] = jnp.where(straight, own[...], passed_ref[...])
    out_ref[:, 256:] = jnp.where(straight, passed_ref[...], own[...])


def merge_last(meta, lam, mine, other, gain, passed):
    return pl.pallas_call(
        merge_last_kernel,
        grid=(1,),
        in_specs=[pl.BlockSpec(memory_space=pltpu.SMEM)] * 2
        + [whole((256, 640))] * 2
        + [whole((1, 256)), whole((256, 256))],
        out_specs=whole((256, 512)),
        out_shape=jax.ShapeDtypeStruct((256, 512), BF16),
        scratch_shapes=[pltpu.VMEM((256, 256), BF16)],
        compiler_params=vmem_params(),
        cost_estimate=cost(1),
        name="merge_last",
    )(meta, lam, mine, other, gain, passed)


def middle_kernel(meta, *refs):
    blocks, mines, others = refs[0:4], refs[4:8], refs[8:11]
    local, gain_ref, normed_ref, own_ref, scratch, power = refs[11:]
    step = pl.program_id(0)
    total = jnp.concatenate([mines[d][256:] for d in (0, 3, 2, 1)], axis=0).astype(F32)
    core = lax.rem(meta[META_Q] // 256, 2)
    rest = pl.ds(pl.multiple_of((1 - (meta[0] ^ core)) * 256, 256), 256)
    for d in range(4):
        rows = blocks[d][...]
        if d:
            rows = jnp.concatenate([rows[64 * d :], rows[: 64 * d]], axis=0)
        for half in range(2):
            block = rows[:, 256 * half : 256 * half + 256]
            if half == 0:
                weights = mines[d][:256]
            else:
                weights = others[d - 1][:256] if d else local[rest, :]
            total += jnp.dot(block, weights, preferred_element_type=F32)
    squares = jnp.sum(total * total, axis=-1, keepdims=True)

    @pl.when(step == 0)
    def _():
        power[...] = jnp.broadcast_to(squares, power.shape)

    @pl.when(step > 0)
    def _():
        power[...] += jnp.broadcast_to(squares, power.shape)

    scratch[step] = total
    own_ref[...] = total[:64]

    @pl.when(step == 3)
    def _():
        root = lax.rsqrt(power[:, :1] * (1.0 / 2048) + EPS)
        for k in range(4):
            cols = slice(512 * k, 512 * k + 512)
            normed_ref[:, cols] = (scratch[k] * root * gain_ref[:, cols]).astype(BF16)


def middle_call(meta, blocks, mines, others, w_out, gain):
    return pl.pallas_call(
        middle_kernel,
        grid=(4,),
        in_specs=[pl.BlockSpec(memory_space=pltpu.SMEM)]
        + [pl.BlockSpec((256, 512), lambda i: (0, 0))] * 4
        + [pl.BlockSpec((320, 512), lambda i: (0, i))] * 7
        + [pl.BlockSpec((512, 512), lambda i: (0, i))]
        + [pl.BlockSpec((1, 2048), lambda i: (0, 0))],
        out_specs=[
            pl.BlockSpec((256, 2048), lambda i: (0, 0)),
            pl.BlockSpec((64, 512), lambda i: (0, i)),
        ],
        out_shape=[jax.ShapeDtypeStruct((256, 2048), BF16), jax.ShapeDtypeStruct((64, 2048), F32)],
        scratch_shapes=[pltpu.VMEM((4, 256, 512), F32), pltpu.VMEM((256, 128), F32)],
        compiler_params=vmem_params(),
        cost_estimate=cost(4),
        name="middle",
    )(meta, *blocks, *mines, *others, w_out, gain)


def ffn_kernel(table, mine_ref, other_ref, *refs):
    pieces = refs[:8]
    keep_ref, send_ref = refs[8:10]
    gu, down, both, hidden, sem = refs[10:]
    for k in range(8):

        def body(i, _, w=pieces[k], base=4 * k):
            row = pl.ds(pl.multiple_of(table[META_W + base + i], 64), 64)
            for n, (start, width) in enumerate(((0, 768), (768, 640))):
                pltpu.make_async_copy(
                    w.at[i, :, pl.ds(start, width)], gu.at[row, pl.ds(start, width)], sem.at[n]
                ).start()
            pltpu.make_async_copy(w.at[i, :, pl.ds(1408, 768)], down.at[row], sem.at[2]).start()
            return 0

        lax.fori_loop(0, 4, body, 0)

    def gate_up(cols):
        both[:256, cols] = jnp.dot(other_ref[...], gu[:, cols], preferred_element_type=F32)
        both[256:, cols] = jnp.dot(mine_ref[...], gu[:, cols], preferred_element_type=F32)

    first, second = gu.at[:, pl.ds(0, 768)], gu.at[:, pl.ds(768, 640)]
    pltpu.make_async_copy(first, first, sem.at[0]).wait()
    gate_up(pl.ds(0, 768))
    pltpu.make_async_copy(second, second, sem.at[1]).wait()
    gate_up(pl.ds(768, 640))

    def activate(k, _):
        rows = pl.ds(pl.multiple_of(k * 128, 128), 128)
        gate, up = both[rows, :704], both[rows, 704:]
        hidden[rows, :704] = (gate / (1.0 + jnp.exp(-gate)) * up).astype(BF16)
        hidden[rows, 704:] = jnp.zeros((128, 64), BF16)
        return 0

    lax.fori_loop(0, 4, activate, 0)
    pltpu.make_async_copy(down, down, sem.at[2]).wait()

    def project(k, _):
        rows = pl.ds(pl.multiple_of(k * 512, 512), 512)
        part = lax.dot_general(
            hidden[...], down[rows, :], (((1,), (1,)), ((), ())), preferred_element_type=F32
        )
        send_ref[:, rows] = part[:256].astype(BF16)
        keep_ref[:, rows] = part[256:]
        return 0

    lax.fori_loop(0, 4, project, 0)


def ffn(table, mine, other, pieces):
    any_space = pl.BlockSpec(memory_space=pl.ANY)
    in_vmem = pl.BlockSpec(memory_space=pltpu.VMEM)
    return pl.pallas_call(
        ffn_kernel,
        in_specs=[pl.BlockSpec(memory_space=pltpu.SMEM), in_vmem, in_vmem] + [any_space] * 8,
        out_specs=[in_vmem] * 2,
        out_shape=[jax.ShapeDtypeStruct((256, 2048), F32), jax.ShapeDtypeStruct((256, 2048), BF16)],
        scratch_shapes=[
            pltpu.VMEM((2048, 1408), BF16),
            pltpu.VMEM((2048, 768), BF16),
            pltpu.VMEM((512, 1408), F32),
            pltpu.VMEM((512, 768), BF16),
            pltpu.SemaphoreType.DMA((3,)),
        ],
        compiler_params=vmem_params(28),
        cost_estimate=cost(9),
        name="ffn",
    )(table, mine, other, *pieces)


def add_kernel(mine_ref, came_ref, middle_ref, own_ref, *sent):
    total = mine_ref[...] + came_ref[...].astype(F32)
    own_ref[...] = total[:64] + middle_ref[...]
    for d in range(3):
        sent[d][...] = total[64 * d + 64 : 64 * d + 128].astype(BF16)


def add_parts(mine, came, middle):
    in_vmem = pl.BlockSpec(memory_space=pltpu.VMEM)
    return pl.pallas_call(
        add_kernel,
        in_specs=[in_vmem] * 3,
        out_specs=[in_vmem] * 4,
        out_shape=[jax.ShapeDtypeStruct((64, 2048), F32)]
        + [jax.ShapeDtypeStruct((64, 2048), BF16)] * 3,
        compiler_params=vmem_params(),
        cost_estimate=cost(1),
        name="add",
    )(mine, came, middle)


def layer(
    stream, queries, keys, values, head_lambda, head_gain, w_out, norm_gain, w_gate, w_up, w_down
):
    sp = lax.axis_index("sp")
    x = lax.axis_index("tp")
    core = sp % 2
    chip = sp // 2
    y = chip % 4
    second = jnp.logical_or(y == 1, y == 2)
    head = second.astype(jnp.int32)

    meta = meta_table(head, x, chip, core)
    own, given = pack(keys, values, queries)
    *kv_held, q_mine = thirds(own, chip_swap(given, STEP["yl"]))
    q_other = core_swap(q_mine)

    w_own, w_given = split_weights(meta, w_gate, w_up, w_down.T)
    w_held = [w_own, core_swap(w_given)]

    line = lines(meta, w_out, stream)
    w_mines = [line] + [shift_x(line, d) for d in (1, 2, 3)]
    for s in range(3):
        kv_far = [chip_swap(kv_held[t], STEP[KV_ORDERS[t][s]]) for t in range(3)]
        if s < 2:
            kv_held = join(kv_held, kv_far)
    states_p = flash(meta, 1, q_mine, q_other, kv_held, [], 5)
    states_o = flash(meta, 0, after(q_mine, *states_p), q_other, kv_held, [], 5)

    def w_step(s, h, array):
        return chip_swap_by_core(array, [STEP[W_ORDERS[c][h][s]] for c in range(2)])

    w_far = [w_step(0, h, w_held[h]) for h in range(2)]
    w_held = join(w_held, w_far)
    w_far = [w_step(1, h, after(w_held[h], *states_p)) for h in range(2)]

    kept, sent = flash(meta, 1, after(q_mine, *states_o), q_other, kv_far, states_p, 5)
    came = core_swap(sent)
    w_held = join([after(w, sent) for w in w_held], w_far)
    w_far = [w_step(2, h, w_held[h]) for h in range(2)]
    w_last1 = w_step(3, 1, w_held[1])
    pair_out = merge(meta, head_lambda, kept, came, head_gain[None])
    passed = chip_swap(pair_out, STEP["yl"])
    w_last0 = w_step(3, 0, after(w_held[0], pair_out))
    kept, sent = flash(meta, 0, after(q_mine, pair_out), q_other, kv_far, states_o, 5)
    came = core_swap(sent)
    block = merge_last(meta, head_lambda, kept, came, head_gain[None], passed)
    blocks = [block] + [shift_x(block, d) for d in (1, 2, 3)]
    w_others = [core_swap(after(w, block)) for w in w_mines[1:]]
    w_tail = [w_step(3, h, after(w_far[h], block)) for h in range(2)]
    w_last = [w_last0, w_last1]
    normed, middle = middle_call(meta, blocks, w_mines, w_others, w_out, norm_gain[None])
    other_normed = core_swap(normed)
    kept_part, sent_part = ffn(
        meta,
        normed,
        other_normed,
        [w_held[0], w_far[0], w_last[0], w_tail[0], w_held[1], w_far[1], w_last[1], w_tail[1]],
    )
    result, *parts = add_parts(kept_part, core_swap(sent_part), middle)
    for d in (1, 2, 3):
        result = result + shift_x(parts[d - 1], d).astype(F32)
    return result.astype(BF16)


def solution(mesh):
    placed = (
        P(("sp", "tp"), None),
        P("sp", "tp"),
        P("sp", "tp"),
        P("sp", "tp"),
        P("tp"),
        P(),
        P("tp", None),
        P(),
        P("sp", "tp"),
        P("sp", "tp"),
        P("tp", "sp"),
    )
    return jax.shard_map(
        layer, mesh=mesh, in_specs=placed, out_specs=P(("sp", "tp"), None), check_vma=False
    )
```

```python
import functools

import jax
import jax.numpy as jnp
import numpy as np
from jax import lax
from jax.experimental import pallas as pl
from jax.experimental.pallas import tpu as pltpu
from jax.sharding import PartitionSpec as P


EPS = 1e-6
NEG = -1e30
F32 = jnp.float32
BF16 = jnp.bfloat16

STEP = {"zl": 4, "zh": 12, "yl": 1, "yh": 3}
KV_ORDERS = (("zl", "zh", "yh"), ("zh", "yh", "zl"), ("yh", "zl", "zh"))
KV_ROWS = (192, 160, 160)
KV_STARTS = (0, 96, 176)
W_ORDERS = (
    (("zl", "yl", "zh", "yh"), ("yl", "zl", "yh", "zh")),
    (("zh", "yh", "zl", "yl"), ("yh", "zh", "yl", "zl")),
)


def patterns(order):
    found = [0]
    for name in order:
        found = found + [p ^ STEP[name] for p in found]
    return found


def chip_swap(array, flip, core_flip=0):
    pairs = [(j * 2 + c, (j ^ flip) * 2 + (c ^ core_flip)) for j in range(16) for c in range(2)]
    return lax.ppermute(array, "sp", pairs)


def chip_swap_by_core(array, flips):
    pairs = [(j * 2 + c, (j ^ flips[c]) * 2 + c) for j in range(16) for c in range(2)]
    return lax.ppermute(array, "sp", pairs)


def core_swap(array):
    return chip_swap(array, 0, 1)


def shift_x(array, d):
    return lax.ppermute(array, "tp", [(i, (i + d) % 4) for i in range(4)])


def meta_layout():
    rows = [[(0, 0, 0, 0, 0)] * 2]
    for core_flip in (0, 1):
        rows.append([(0, 0, core_flip, 256, 0), (STEP["yl"],) * 2 + (core_flip, 256, 0)])
    for far in (0, 1):
        for t in range(3):
            for p in patterns(KV_ORDERS[t])[4 * far : 4 * far + 4]:
                rows.append(
                    [(p, p, 0, 256, KV_STARTS[t]), (p ^ STEP["yl"],) * 2 + (0, 256, KV_STARTS[t])]
                )
    for h in range(2):
        rows.append(
            [(a, b, h, 64, 0) for a, b in zip(patterns(W_ORDERS[0][h]), patterns(W_ORDERS[1][h]))]
        )
    return np.array([entry for row in rows for entry in row], np.int32)


META_Q, META_K, META_W = 2, 6, 54


def meta_table(head, x, chip, core):
    flip0, flip1, core_flip, factor, addend = (jnp.asarray(v) for v in meta_layout().T)
    flip = jnp.where(core == 0, flip0, flip1)
    table = ((chip ^ flip) * 2 + (core ^ core_flip)) * factor + addend
    place = jnp.arange(table.shape[0])
    table = jnp.where(place == 0, head, jnp.where(place == 1, x, table))
    return table.astype(jnp.int32)


def after(value, *others):
    return lax.optimization_barrier((value, others))[0]


def whole(shape):
    return pl.BlockSpec(shape, lambda *_: (0,) * len(shape))


def cost(us):
    return pl.CostEstimate(flops=int(us * 1e9), bytes_accessed=int(1e5), transcendentals=0)


def vmem_params(mib=16, **kw):
    return pltpu.CompilerParams(vmem_limit_bytes=mib << 20, **kw)


def pack_kernel(keys, values, queries, own_ref, given_ref, ins, outs, sem):
    y, x = lax.rem(lax.axis_index("sp") // 2, 4), lax.axis_index("tp")
    second = jnp.where((y == 1) | (y == 2), 1, 0)
    loads = [
        pltpu.make_async_copy(ref, ins.at[k], sem.at[k])
        for k, ref in enumerate((keys, values, queries))
    ]
    stores = [
        pltpu.make_async_copy(outs.at[k], ref, sem.at[3 + k])
        for k, ref in enumerate((given_ref, own_ref))
    ]
    for load in loads:
        load.start()
    for load in loads:
        load.wait()
    for k, turn in enumerate((1 - second, second)):
        cols = pl.ds(pl.multiple_of(turn * 256, 256), 256)
        outs[k, :, :256] = ins[0, :, cols]
        outs[k, :, 256:512] = ins[1, :, cols]
        for j in range(4):
            rows = pl.ds(pl.multiple_of(lax.rem(x + j, 4) * 64, 64), 64)
            outs[k, 64 * j : 64 * j + 64, 512:] = ins[2, rows, cols]
        stores[k].start()
    for store in stores:
        store.wait()


def pack(keys, values, queries):
    in_hbm = pl.BlockSpec(memory_space=pltpu.HBM)
    return pl.pallas_call(
        pack_kernel,
        in_specs=[in_hbm] * 3,
        out_specs=[in_hbm] * 2,
        out_shape=[jax.ShapeDtypeStruct((256, 768), BF16)] * 2,
        scratch_shapes=[
            pltpu.VMEM((3, 256, 512), BF16),
            pltpu.VMEM((2, 256, 768), BF16),
            pltpu.SemaphoreType.DMA((5,)),
        ],
        compiler_params=vmem_params(63),
        cost_estimate=cost(1),
        name="pack",
    )(keys, values, queries)


def weights_kernel(meta, gate, up, down, own_ref, given_ref):
    first = lax.rem(meta[META_Q] // 256, 2) == 0
    for k in range(2):
        cols = slice(704 * k, 704 * k + 704)
        block = jnp.concatenate(
            [gate[:, cols], up[:, cols], down[:, cols], jnp.zeros((64, 64), BF16)], axis=1
        )

        @pl.when(first == (k == 0))
        def _():
            own_ref[0] = block

        @pl.when(first != (k == 0))
        def _():
            given_ref[0] = block


def split_weights(meta, gate, up, down):
    return pl.pallas_call(
        weights_kernel,
        grid=(1,),
        in_specs=[pl.BlockSpec(memory_space=pltpu.SMEM)] + [whole((64, 1408))] * 3,
        out_specs=[whole((1, 64, 2176))] * 2,
        out_shape=[jax.ShapeDtypeStruct((1, 64, 2176), BF16)] * 2,
        compiler_params=vmem_params(63),
        cost_estimate=cost(2),
        name="weights",
    )(meta, gate, up, down)


def lines_kernel(meta, w_out, stream, out_ref, held, sem):
    half = pl.multiple_of((meta[0] ^ lax.rem(meta[META_Q] // 256, 2)) * 256, 256)
    loads = [
        pltpu.make_async_copy(w_out.at[pl.ds(half, 256)], held.at[pl.ds(0, 256)], sem.at[0]),
        pltpu.make_async_copy(stream, held.at[pl.ds(256, 64)], sem.at[1]),
    ]
    for load in loads:
        load.start()
    for load in loads:
        load.wait()
    store = pltpu.make_async_copy(held, out_ref, sem.at[2])
    store.start()
    store.wait()


def lines(meta, w_out, stream):
    in_hbm = pl.BlockSpec(memory_space=pltpu.HBM)
    return pl.pallas_call(
        lines_kernel,
        in_specs=[pl.BlockSpec(memory_space=pltpu.SMEM)] + [in_hbm] * 2,
        out_specs=in_hbm,
        out_shape=jax.ShapeDtypeStruct((320, 2048), BF16),
        scratch_shapes=[pltpu.VMEM((320, 2048), BF16), pltpu.SemaphoreType.DMA((3,))],
        compiler_params=vmem_params(63),
        cost_estimate=cost(2),
        name="lines",
    )(meta, w_out, stream)


def thirds_kernel(own, taken, *outs):
    for t in range(3):
        half, start = KV_ROWS[t] // 2, KV_STARTS[t]
        outs[t][0, :half] = own[start : start + half, :512]
        outs[t][0, half:] = taken[start : start + half, :512]
    outs[3][:256] = own[:, 512:]
    outs[3][256:] = taken[:, 512:]


def thirds(own, taken):
    shapes = [(1, n, 512) for n in KV_ROWS] + [(512, 256)]
    return pl.pallas_call(
        thirds_kernel,
        grid=(1,),
        in_specs=[whole((256, 768))] * 2,
        out_specs=[whole(shape) for shape in shapes],
        out_shape=[jax.ShapeDtypeStruct(shape, BF16) for shape in shapes],
        compiler_params=vmem_params(16),
        cost_estimate=cost(1),
        name="thirds",
    )(own, taken)


def join_kernel(count, *refs):
    for k in range(count):
        n = refs[k].shape[0]
        refs[2 * count + k][:n] = refs[k][...]
        refs[2 * count + k][n:] = refs[count + k][...]


def join(held, far):
    shapes = [(2 * a.shape[0], *a.shape[1:]) for a in held]
    return pl.pallas_call(
        functools.partial(join_kernel, len(held)),
        grid=(1,),
        in_specs=[whole(a.shape) for a in (*held, *far)],
        out_specs=[whole(shape) for shape in shapes],
        out_shape=[jax.ShapeDtypeStruct(shape, BF16) for shape in shapes],
        compiler_params=vmem_params(),
        cost_estimate=cost(1),
        name="join",
    )(*held, *far)


def flash_first_kernel(block, scale, meta, *refs):
    kv_refs, rest = refs[2:5], refs[5:]
    row = lax.broadcasted_iota(jnp.int32, (512, 1), 0)
    qpos = (
        jnp.where(row < 256, meta[META_Q + block], meta[META_Q + block + 2])
        + ((meta[1] + (row >> 6)) & 3) * 64
        + (row & 63)
    )
    queries = jnp.concatenate([refs[0][...], refs[1][...]], axis=0)
    state = []
    for _ in range(2):
        state.append(
            (jnp.full((512, 1), NEG, F32), jnp.zeros((512, 1), F32), jnp.zeros((512, 256), F32))
        )
    for t in range(3):
        kv_ref, half = kv_refs[t], KV_ROWS[t] // 2
        key = lax.broadcasted_iota(jnp.int32, (1, 8 * half), 1)
        kpos = key
        for k in range(8):
            base = meta[META_K + 8 * t + k]
            kpos = jnp.where(key >= k * half, base + key - k * half, kpos)
        visible = kpos <= qpos
        for s in range(2):
            top, total, acc = state[s]
            scores = lax.dot_general(
                queries[:, 128 * s : 128 * s + 128],
                kv_ref[:, 128 * s : 128 * s + 128],
                (((1,), (1,)), ((), ())),
                preferred_element_type=F32,
            )
            scores = jnp.where(visible, scores, NEG)
            new_top = jnp.maximum(top, jnp.max(scores, axis=1, keepdims=True))
            weights = jnp.exp2((scores - new_top) * scale)
            fade = jnp.exp2((top - new_top) * scale)
            total = total * fade + jnp.sum(weights, axis=1, keepdims=True)
            acc = acc * fade + jnp.dot(
                weights.astype(BF16), kv_ref[:, 256:512], preferred_element_type=F32
            )
            state[s] = (new_top, total, acc)
    lane = lax.broadcasted_iota(jnp.int32, (256, 128), 1)
    for k in range(2):
        out_ref = rest[k - 2]
        rows = slice(256 * k, 256 * k + 256)
        tail = jnp.zeros((256, 128), F32)
        for s in range(2):
            top, total, acc = (part[rows] for part in state[s])
            cols = slice(256 * s, 256 * s + 256)
            out_ref[:, cols] = acc
            tail = jnp.where(lane == s, top, tail)
            tail = jnp.where(lane == 2 + s, total, tail)
        out_ref[:, 512:640] = tail


def flash_last_kernel(block, scale, meta, *refs):
    kv_refs, rest = refs[2:5], refs[5:]
    step = pl.program_id(0)
    row = lax.broadcasted_iota(jnp.int32, (256, 1), 0)
    qpos = (
        meta[META_Q + block + 2 * step] + ((meta[1] + (row >> 6)) & 3) * 64 + (row & 63)
    )
    queries = jnp.where(step == 0, refs[0][...], refs[1][...])
    state = []
    for _ in range(2):
        state.append(
            (jnp.full((256, 1), NEG, F32), jnp.zeros((256, 1), F32), jnp.zeros((256, 256), F32))
        )
    for t in range(3):
        kv_ref, half = kv_refs[t], KV_ROWS[t] // 2
        key = lax.broadcasted_iota(jnp.int32, (1, 8 * half), 1)
        kpos = key
        for k in range(8):
            base = meta[META_K + 24 + 8 * t + k]
            kpos = jnp.where(key >= k * half, base + key - k * half, kpos)
        visible = kpos <= qpos
        for s in range(2):
            top, total, acc = state[s]
            scores = lax.dot_general(
                queries[:, 128 * s : 128 * s + 128],
                kv_ref[:, 128 * s : 128 * s + 128],
                (((1,), (1,)), ((), ())),
                preferred_element_type=F32,
            )
            scores = jnp.where(visible, scores, NEG)
            new_top = jnp.maximum(top, jnp.max(scores, axis=1, keepdims=True))
            weights = jnp.exp2((scores - new_top) * scale)
            fade = jnp.exp2((top - new_top) * scale)
            total = total * fade + jnp.sum(weights, axis=1, keepdims=True)
            acc = acc * fade + jnp.dot(
                weights.astype(BF16), kv_ref[:, 256:512], preferred_element_type=F32
            )
            state[s] = (new_top, total, acc)
    lane = lax.broadcasted_iota(jnp.int32, (256, 128), 1)
    for k in range(2):

        @pl.when(step == k)
        def _():
            out_ref = rest[k - 2]
            near = rest[k]
            ends = jnp.zeros((256, 128), F32)
            for s in range(2):
                top, total, acc = state[s]
                near_top = near[:, 512 + s : 513 + s]
                both_top = jnp.maximum(top, near_top)
                fade = jnp.exp2((top - both_top) * scale)
                near_fade = jnp.exp2((near_top - both_top) * scale)
                total = total * fade + near[:, 514 + s : 515 + s] * near_fade
                cols = slice(256 * s, 256 * s + 256)
                out_ref[:, cols] = acc * fade + near[:, cols] * near_fade
                ends = jnp.where(lane == s, both_top, ends)
                ends = jnp.where(lane == 2 + s, total, ends)
            out_ref[:, 512:640] = ends


def flash(meta, block, q_mine, q_other, kvs, states, us):
    scale = float(128**-0.5 * np.log2(np.e))
    kvs = [a.reshape(-1, 512) for a in kvs]
    return pl.pallas_call(
        functools.partial(flash_last_kernel if states else flash_first_kernel, block, scale),
        grid=(2,) if states else (1,),
        in_specs=[pl.BlockSpec(memory_space=pltpu.SMEM)]
        + [pl.BlockSpec((256, 256), lambda i: (block, 0))] * 2
        + [whole(a.shape) for a in kvs]
        + [whole((256, 640))] * len(states),
        out_specs=[whole((256, 640))] * 2,
        out_shape=[jax.ShapeDtypeStruct((256, 640), F32)] * 2,
        compiler_params=vmem_params(),
        cost_estimate=cost(us),
        name="flash",
    )(meta, q_mine, q_other, *kvs, *states)


def merge_kernel(meta, lam, mine_ref, other_ref, gain_ref, out_ref):
    scale = float(128**-0.5 * np.log2(np.e))
    maps = []
    for s in range(2):
        top_a, top_b = mine_ref[:, 512 + s : 513 + s], other_ref[:, 512 + s : 513 + s]
        top = jnp.maximum(top_a, top_b)
        fade_a, fade_b = jnp.exp2((top_a - top) * scale), jnp.exp2((top_b - top) * scale)
        total = mine_ref[:, 514 + s : 515 + s] * fade_a + other_ref[:, 514 + s : 515 + s] * fade_b
        cols = slice(256 * s, 256 * s + 256)
        maps.append((mine_ref[:, cols] * fade_a + other_ref[:, cols] * fade_b) / total)
    contrast = maps[0] - lax.select(meta[0] == 1, lam[1], lam[0]) * maps[1]
    power = jnp.mean(contrast * contrast, axis=-1, keepdims=True)
    out_ref[...] = (contrast * lax.rsqrt(power + EPS) * gain_ref[...]).astype(BF16)


def merge(meta, lam, mine, other, gain):
    return pl.pallas_call(
        merge_kernel,
        grid=(1,),
        in_specs=[pl.BlockSpec(memory_space=pltpu.SMEM)] * 2
        + [whole((256, 640))] * 2
        + [whole((1, 256))],
        out_specs=whole((256, 256)),
        out_shape=jax.ShapeDtypeStruct((256, 256), BF16),
        compiler_params=vmem_params(),
        cost_estimate=cost(1),
        name="merge",
    )(meta, lam, mine, other, gain)


def merge_last_kernel(meta, lam, mine_ref, other_ref, gain_ref, passed_ref, out_ref, own):
    merge_kernel(meta, lam, mine_ref, other_ref, gain_ref, own)
    straight = lax.rem(meta[META_Q] // 256, 2) == 0
    out_ref[:, :256] = jnp.where(straight, own[...], passed_ref[...])
    out_ref[:, 256:] = jnp.where(straight, passed_ref[...], own[...])


def merge_last(meta, lam, mine, other, gain, passed):
    return pl.pallas_call(
        merge_last_kernel,
        grid=(1,),
        in_specs=[pl.BlockSpec(memory_space=pltpu.SMEM)] * 2
        + [whole((256, 640))] * 2
        + [whole((1, 256)), whole((256, 256))],
        out_specs=whole((256, 512)),
        out_shape=jax.ShapeDtypeStruct((256, 512), BF16),
        scratch_shapes=[pltpu.VMEM((256, 256), BF16)],
        compiler_params=vmem_params(),
        cost_estimate=cost(1),
        name="merge_last",
    )(meta, lam, mine, other, gain, passed)


def middle_kernel(meta, *refs):
    blocks, mines, others = refs[0:4], refs[4:8], refs[8:11]
    local, gain_ref, normed_ref, own_ref, scratch, power = refs[11:]
    step = pl.program_id(0)
    total = jnp.concatenate([mines[d][256:] for d in (0, 3, 2, 1)], axis=0).astype(F32)
    core = lax.rem(meta[META_Q] // 256, 2)
    rest = pl.ds(pl.multiple_of((1 - (meta[0] ^ core)) * 256, 256), 256)
    for d in range(4):
        rows = blocks[d][...]
        if d:
            rows = jnp.concatenate([rows[64 * d :], rows[: 64 * d]], axis=0)
        for half in range(2):
            block = rows[:, 256 * half : 256 * half + 256]
            if half == 0:
                weights = mines[d][:256]
            else:
                weights = others[d - 1][:256] if d else local[rest, :]
            total += jnp.dot(block, weights, preferred_element_type=F32)
    squares = jnp.sum(total * total, axis=-1, keepdims=True)

    @pl.when(step == 0)
    def _():
        power[...] = jnp.broadcast_to(squares, power.shape)

    @pl.when(step > 0)
    def _():
        power[...] += jnp.broadcast_to(squares, power.shape)

    scratch[step] = total
    own_ref[...] = total[:64]

    @pl.when(step == 3)
    def _():
        root = lax.rsqrt(power[:, :1] * (1.0 / 2048) + EPS)
        for k in range(4):
            cols = slice(512 * k, 512 * k + 512)
            normed_ref[:, cols] = (scratch[k] * root * gain_ref[:, cols]).astype(BF16)


def middle_call(meta, blocks, mines, others, w_out, gain):
    return pl.pallas_call(
        middle_kernel,
        grid=(4,),
        in_specs=[pl.BlockSpec(memory_space=pltpu.SMEM)]
        + [pl.BlockSpec((256, 512), lambda i: (0, 0))] * 4
        + [pl.BlockSpec((320, 512), lambda i: (0, i))] * 7
        + [pl.BlockSpec((512, 512), lambda i: (0, i))]
        + [pl.BlockSpec((1, 2048), lambda i: (0, 0))],
        out_specs=[
            pl.BlockSpec((256, 2048), lambda i: (0, 0)),
            pl.BlockSpec((64, 512), lambda i: (0, i)),
        ],
        out_shape=[jax.ShapeDtypeStruct((256, 2048), BF16), jax.ShapeDtypeStruct((64, 2048), F32)],
        scratch_shapes=[pltpu.VMEM((4, 256, 512), F32), pltpu.VMEM((256, 128), F32)],
        compiler_params=vmem_params(),
        cost_estimate=cost(4),
        name="middle",
    )(meta, *blocks, *mines, *others, w_out, gain)


def ffn_kernel(table, mine_ref, other_ref, *refs):
    pieces = refs[:8]
    send_ref, hidden, down = refs[8:11]
    gu, both, sem = refs[11:]
    for k in range(8):

        def body(i, _, w=pieces[k], base=4 * k):
            row = pl.ds(pl.multiple_of(table[META_W + base + i], 64), 64)
            for n, (start, width) in enumerate(((0, 768), (768, 640))):
                pltpu.make_async_copy(
                    w.at[i, :, pl.ds(start, width)], gu.at[row, pl.ds(start, width)], sem.at[n]
                ).start()
            pltpu.make_async_copy(w.at[i, :, pl.ds(1408, 768)], down.at[row], sem.at[2]).start()
            return 0

        lax.fori_loop(0, 4, body, 0)

    def gate_up(cols):
        both[:256, cols] = jnp.dot(other_ref[...], gu[:, cols], preferred_element_type=F32)
        both[256:, cols] = jnp.dot(mine_ref[...], gu[:, cols], preferred_element_type=F32)

    first, second = gu.at[:, pl.ds(0, 768)], gu.at[:, pl.ds(768, 640)]
    pltpu.make_async_copy(first, first, sem.at[0]).wait()
    gate_up(pl.ds(0, 768))
    pltpu.make_async_copy(second, second, sem.at[1]).wait()
    gate_up(pl.ds(768, 640))

    def activate(k, _):
        rows = pl.ds(pl.multiple_of(k * 128, 128), 128)
        gate, up = both[rows, :704], both[rows, 704:]
        hidden[rows, :704] = (gate / (1.0 + jnp.exp(-gate)) * up).astype(BF16)
        hidden[rows, 704:] = jnp.zeros((128, 64), BF16)
        return 0

    lax.fori_loop(0, 4, activate, 0)
    pltpu.make_async_copy(down, down, sem.at[2]).wait()

    project_rows(hidden, 0, down, send_ref)


def project_rows(hidden, first, down, out_ref):
    def project(k, _):
        rows = pl.ds(pl.multiple_of(k * 512, 512), 512)
        part = lax.dot_general(
            hidden[first : first + 256],
            down[rows, :],
            (((1,), (1,)), ((), ())),
            preferred_element_type=F32,
        )
        out_ref[:, rows] = part.astype(out_ref.dtype)
        return 0

    lax.fori_loop(0, 4, project, 0)


def ffn(table, mine, other, pieces):
    any_space = pl.BlockSpec(memory_space=pl.ANY)
    in_vmem = pl.BlockSpec(memory_space=pltpu.VMEM)
    return pl.pallas_call(
        ffn_kernel,
        in_specs=[pl.BlockSpec(memory_space=pltpu.SMEM), in_vmem, in_vmem] + [any_space] * 8,
        out_specs=[in_vmem] * 3,
        out_shape=[
            jax.ShapeDtypeStruct((256, 2048), BF16),
            jax.ShapeDtypeStruct((512, 768), BF16),
            jax.ShapeDtypeStruct((2048, 768), BF16),
        ],
        scratch_shapes=[
            pltpu.VMEM((2048, 1408), BF16),
            pltpu.VMEM((512, 1408), F32),
            pltpu.SemaphoreType.DMA((3,)),
        ],
        compiler_params=vmem_params(28),
        cost_estimate=cost(9),
        name="ffn",
    )(table, mine, other, *pieces)


def own_rows_kernel(hidden, down, out_ref):
    project_rows(hidden, 256, down, out_ref)


def own_rows(hidden, down):
    in_vmem = pl.BlockSpec(memory_space=pltpu.VMEM)
    return pl.pallas_call(
        own_rows_kernel,
        in_specs=[in_vmem] * 2,
        out_specs=in_vmem,
        out_shape=jax.ShapeDtypeStruct((256, 2048), F32),
        compiler_params=vmem_params(),
        cost_estimate=cost(2),
        name="own_rows",
    )(hidden, down)


def add_kernel(mine_ref, came_ref, middle_ref, own_ref, *sent):
    total = mine_ref[...] + came_ref[...].astype(F32)
    own_ref[...] = total[:64] + middle_ref[...]
    for d in range(3):
        sent[d][...] = total[64 * d + 64 : 64 * d + 128].astype(BF16)


def add_parts(mine, came, middle):
    in_vmem = pl.BlockSpec(memory_space=pltpu.VMEM)
    return pl.pallas_call(
        add_kernel,
        in_specs=[in_vmem] * 3,
        out_specs=[in_vmem] * 4,
        out_shape=[jax.ShapeDtypeStruct((64, 2048), F32)]
        + [jax.ShapeDtypeStruct((64, 2048), BF16)] * 3,
        compiler_params=vmem_params(),
        cost_estimate=cost(1),
        name="add",
    )(mine, came, middle)


def layer(
    stream, queries, keys, values, head_lambda, head_gain, w_out, norm_gain, w_gate, w_up, w_down
):
    sp = lax.axis_index("sp")
    x = lax.axis_index("tp")
    core = sp % 2
    chip = sp // 2
    y = chip % 4
    second = jnp.logical_or(y == 1, y == 2)
    head = second.astype(jnp.int32)

    meta = meta_table(head, x, chip, core)
    own, given = pack(keys, values, queries)
    *kv_held, q_mine = thirds(own, chip_swap(given, STEP["yl"]))
    q_other = core_swap(q_mine)

    w_own, w_given = split_weights(meta, w_gate, w_up, w_down.T)
    w_held = [w_own, core_swap(w_given)]

    line = lines(meta, w_out, stream)
    w_mines = [line] + [shift_x(line, d) for d in (1, 2, 3)]
    for s in range(3):
        kv_far = [chip_swap(kv_held[t], STEP[KV_ORDERS[t][s]]) for t in range(3)]
        if s < 2:
            kv_held = join(kv_held, kv_far)
    states_p = flash(meta, 1, q_mine, q_other, kv_held, [], 5)
    states_o = flash(meta, 0, after(q_mine, *states_p), q_other, kv_held, [], 5)

    def w_step(s, h, array):
        return chip_swap_by_core(array, [STEP[W_ORDERS[c][h][s]] for c in range(2)])

    w_far = [w_step(0, h, w_held[h]) for h in range(2)]
    w_held = join(w_held, w_far)
    w_far = [w_step(1, h, after(w_held[h], *states_p)) for h in range(2)]

    kept, sent = flash(meta, 1, after(q_mine, *states_o), q_other, kv_far, states_p, 5)
    came = core_swap(sent)
    w_held = join([after(w, sent) for w in w_held], w_far)
    w_far = [w_step(2, h, w_held[h]) for h in range(2)]
    w_last1 = w_step(3, 1, w_held[1])
    pair_out = merge(meta, head_lambda, kept, came, head_gain[None])
    passed = chip_swap(pair_out, STEP["yl"])
    w_last0 = w_step(3, 0, after(w_held[0], pair_out))
    kept, sent = flash(meta, 0, after(q_mine, pair_out), q_other, kv_far, states_o, 5)
    came = core_swap(sent)
    block = merge_last(meta, head_lambda, kept, came, head_gain[None], passed)
    blocks = [block] + [shift_x(block, d) for d in (1, 2, 3)]
    w_others = [core_swap(after(w, block)) for w in w_mines[1:]]
    w_tail = [w_step(3, h, after(w_far[h], block)) for h in range(2)]
    w_last = [w_last0, w_last1]
    normed, middle = middle_call(meta, blocks, w_mines, w_others, w_out, norm_gain[None])
    other_normed = core_swap(normed)
    sent_part, hidden, down = ffn(
        meta,
        normed,
        other_normed,
        [w_held[0], w_far[0], w_last[0], w_tail[0], w_held[1], w_far[1], w_last[1], w_tail[1]],
    )
    came_part = core_swap(sent_part)
    kept_part = own_rows(hidden, down)
    result, *parts = add_parts(kept_part, came_part, middle)
    for d in (1, 2, 3):
        result = result + shift_x(parts[d - 1], d).astype(F32)
    return result.astype(BF16)


def solution(mesh):
    placed = (
        P(("sp", "tp"), None),
        P("sp", "tp"),
        P("sp", "tp"),
        P("sp", "tp"),
        P("tp"),
        P(),
        P("tp", None),
        P(),
        P("sp", "tp"),
        P("sp", "tp"),
        P("tp", "sp"),
    )
    return jax.shard_map(
        layer, mesh=mesh, in_specs=placed, out_specs=P(("sp", "tp"), None), check_vma=False
    )
```
